32 devices in a mesh: sp: 16 (over z, y, core), tp: 2 (over x).
Axes of the slice: x: 2, y: 2, z: 4, core: 2. Of those that a mesh axis runs over, the one named last changes fastest.
Arguments:
- pool_input: bfloat16 [4, 128, 8192], P(None, 'tp', 'sp'), may hold values from -8 to 8
- doc_ids: int32 [8192], P('sp'), may hold values from 0 to 3, never falling along the last dimension, each value on 1 to 4096 neighbouring positions
- pool_map: bfloat16 [4, 128, 128], replicated, may hold values from -0.5 to 0.5
- pool_scale: float32 [512], replicated, may hold values from 0.1 to 1.9
- w_out: bfloat16 [512, 2048], replicated, may hold values from -0.25 to 0.25
- residual: bfloat16 [8192, 2048], P(('sp', 'tp')), may hold values from -6 to 6
- mix_gain: float32 [2048], replicated, may hold values from 0.1 to 1.9
- ffn_gain: float32 [2048], replicated, may hold values from 0.1 to 1.9
- out_gain: float32 [2048], replicated, may hold values from 0.1 to 1.9
- expert_ids: int32 [8192, 2], P(('sp', 'tp')), may hold values from 0 to 31, all different within a row; in each aligned block of 256 rows (0 to 255, 256 to 511, ...) at most 32 rows name the same one
- route_logits: float32 [8192, 2], P(('sp', 'tp')), may hold values from -6 to 6
- w_gate: bfloat16 [32, 2048, 1024], P(('sp', 'tp')), may hold values from -0.125 to 0.125
- w_up: bfloat16 [32, 2048, 1024], P(('sp', 'tp')), may hold values from -0.125 to 0.125
- w_down: bfloat16 [32, 1024, 2048], P(('sp', 'tp')), may hold values from -0.1875 to 0.1875
Outputs:
- layer_out: bfloat16 [8192, 2048], P(('sp', 'tp'))
The draws below stay inside these ranges and needn't reach their ends.
Inputs may be any that keep to these rules, and one draw needn't show every extreme that they name: `doc_ids`: document numbers never fall along the positions; no document has more than 4096 positions. `expert_ids`: each row names 2 different experts; within each aligned block of 256 rows no expert is named by more than 32 rows, a bound that some block reaches.
All inputs are finite; a program needn't handle non-finite values.
Results may differ from the reference program's by a relative error of at most 0.03.
Values may be sent and summed in bfloat16 or wider, within the bound.
A program may use at most 64 MiB of HBM per device.

```python
import math
import jax
import jax.numpy as jnp
import numpy as np
from jax import lax

D = 2048
FF = 1024
GROUPS = 4
GROUP_W = 128
TOP_K = 2
TOK_DEV = 512
POOL_W = 512
TOKENS = 8192
ROWS_DEV = 256
EXPERTS = 32
CAP = 32
DOCS = 4
DOC_MOST = 4096
DEVICES = 32


def draw_pool_input(key, part):
    noise_key = jax.random.fold_in(key, 11)
    level_key = jax.random.fold_in(key, 12)
    span_len = max(TOK_DEV // 2, 1)
    span_count = TOKENS // span_len
    noise = jax.random.normal(noise_key, (GROUPS, GROUP_W, TOKENS), jnp.float32)
    levels = jax.random.normal(level_key, (GROUPS, GROUP_W, span_count), jnp.float32)
    full = noise + jnp.repeat(levels, span_len, axis=2)
    return jnp.clip(full, -8.0, 8.0).astype(jnp.bfloat16)


def block_scale(key, extent, pieces, low, largest):
    def one(dim, parts):
        heights = jax.random.uniform(jax.random.fold_in(jax.random.fold_in(key, 6), dim), (parts,), jnp.float32, low / len(pieces), largest / len(pieces))
        return jnp.repeat(jnp.exp(heights), extent[dim] // parts).reshape((-1,) + (1,) * (len(extent) - dim - 1))

    loudness = one(*pieces[0])
    for cut in pieces[1:]:
        loudness = loudness * one(*cut)
    return loudness


def split_up(count, total, reach, lean):
    loads = [(1 << 20) // math.isqrt(rank ** lean) + 1 for rank in range(2, count + 1)]
    surplus, given = total - reach - (count - 1), [1] * (count - 1)
    while surplus > 0:
        candidates = [i for i in range(count - 1) if given[i] < reach]
        whole, remaining = sum([loads[i] for i in candidates]), surplus
        for i in candidates:
            addition = min(reach - given[i], max(1, remaining * loads[i] // whole), surplus)
            given[i] = given[i] + addition
            surplus = surplus - addition
    return np.array([reach] + given)


def uneven_parts(own_key, number_of, total, bound, lean):
    if number_of == 2:
        one = jax.random.randint(own_key, (), max(1, total - bound), min(bound, total - 1) + 1)
        return jnp.stack([one, total - one])
    tallies = jnp.asarray(split_up(number_of, total, bound, lean), jnp.int32)
    pairs = (number_of - 1) // 2
    giver, sink = tallies[1:1 + 2 * pairs:2], tallies[2:2 + 2 * pairs:2]
    room = jnp.minimum(giver - 1, bound - sink)
    passed = jax.random.randint(jax.random.fold_in(own_key, 1), (pairs,), 0, 1 << 20) % (room + 1)
    tallies = tallies.at[1:1 + 2 * pairs:2].set(giver - passed).at[2:2 + 2 * pairs:2].set(sink + passed)
    return tallies[jax.random.permutation(jax.random.fold_in(own_key, 2), number_of)]


def deal_out(rng, own, number, rows, amount, top, limit, slope):
    order = jax.random.permutation(rng, amount)
    crowded, ordinary = portions_of(amount, rows * top, limit, slope, True), portions_of(amount, rows * top, limit, slope, False)
    places = jnp.arange(amount)

    def named(sizes, rotation):
        used = int((sizes > 0).sum())
        fixed = max(1, used // 4)
        moved = fixed + (places - fixed + rotation * (used - fixed)) % max(1, amount - fixed)
        return jnp.zeros((amount,), jnp.int32).at[order[jnp.where(places < fixed, places, moved)]].set(jnp.asarray(sizes, jnp.int32))

    sizes = jnp.where(number % 4 == 0, named(crowded, number // 4), named(ordinary, number - number // 4 - 1))
    mixed = jax.random.permutation(jax.random.fold_in(own, 3), amount)
    donor, taker = mixed[0:amount // 2 * 2:2], mixed[1:amount // 2 * 2:2]
    margin = jnp.minimum(sizes[donor] - 1, limit - sizes[taker]) // 2
    margin = jnp.where((donor == order[0]) | (taker == order[0]) | (sizes[taker] == 0), 0, jnp.maximum(margin, 0))
    moved = jax.random.randint(jax.random.fold_in(own, 4), (amount // 2,), 0, 1 << 20) % (margin + 1)
    sizes = sizes.at[donor].add(-moved).at[taker].add(moved)
    members = jnp.searchsorted(jnp.cumsum(sizes), jnp.arange(rows * top), side="right").astype(jnp.int32)
    table = members.reshape(top, rows).T
    table = table[jax.random.permutation(jax.random.fold_in(own, 1), rows)]
    rotation = jax.random.randint(jax.random.fold_in(own, 2), (rows, 1), 0, top)
    return jnp.take_along_axis(table, (jnp.arange(top)[None, :] + rotation) % top, axis=1)


def portions_of(number_of, total, bound, lean, full):
    loads = [(1 << 20) // math.isqrt(rank ** lean) + 1 for rank in range(1, number_of + 1)]
    largest = bound if full else min(bound, max(-(-total // number_of), total * loads[0] // sum(loads)))
    least = 1 if total - largest >= number_of - 1 else 0
    holding, spare = [largest] + [least] * (number_of - 1), total - largest - least * (number_of - 1)
    while spare > 0:
        free = [i for i in range(1, number_of) if holding[i] < largest] or [i for i in range(1, number_of) if holding[i] < bound]
        pool, remaining = sum([loads[i] for i in free]), spare
        for i in free:
            addition = min(bound - holding[i], max(1, remaining * loads[i] // pool), spare)
            holding[i] = holding[i] + addition
            spare = spare - addition
    return np.array(holding)


def scatter_about(rng, dims, width, reach, pieces=(), kind=jnp.bfloat16):
    loudness = block_scale(rng, dims, pieces, -0.22, 0.18) if pieces else 1.0
    array = jax.random.normal(rng, dims, jnp.float32) * width * loudness
    return jnp.minimum(jnp.maximum(array, -reach), reach).astype(kind)


def setup_inputs(seed: int = 0) -> dict:
    keys = jax.random.split(jax.random.key(seed), 15)
    pool_input = draw_pool_input(jax.random.fold_in(keys[14], 71), 0)
    doc_ids = jnp.searchsorted(jnp.cumsum(uneven_parts(keys[1], DOCS, TOKENS, DOC_MOST, 2)), jnp.arange(TOKENS), side="right").astype(jnp.int32)
    pool_map = scatter_about(keys[2], (GROUPS, GROUP_W, GROUP_W), GROUP_W ** -0.5, 0.5)
    pool_scale = jnp.clip(1.0 + 0.18 * jax.random.normal(keys[3], (POOL_W,), jnp.float32), 0.1, 1.9)
    w_out = scatter_about(keys[4], (POOL_W, D), POOL_W ** -0.5, 0.25)
    residual = scatter_about(keys[5], (TOKENS, D), 1.0, 6.0, ((0, 32),))
    mix_gain = jnp.clip(1.0 + 0.18 * jax.random.normal(keys[6], (D,), jnp.float32), 0.1, 1.9)
    ffn_gain = jnp.clip(1.0 + 0.18 * jax.random.normal(keys[7], (D,), jnp.float32), 0.1, 1.9)
    out_gain = jnp.clip(1.0 + 0.18 * jax.random.normal(keys[8], (D,), jnp.float32), 0.1, 1.9)
    expert_ids_keys = jax.random.split(jax.random.fold_in(keys[9], 1), TOKENS // ROWS_DEV)
    expert_ids_turns = jax.random.permutation(jax.random.fold_in(keys[9], 3), TOKENS // ROWS_DEV)
    expert_ids = jax.vmap(lambda own, number: deal_out(jax.random.fold_in(keys[9], 2), own, number, ROWS_DEV, EXPERTS, TOP_K, CAP, 2))(expert_ids_keys, expert_ids_turns).reshape((TOKENS, TOP_K))
    route_logits = scatter_about(keys[10], (TOKENS, TOP_K), 1.5, 6.0, ((0, 32),), jnp.float32)
    w_gate = scatter_about(keys[11], (EXPERTS, D, FF), D ** -0.5, 0.125, ((0, 32),))
    w_up = scatter_about(keys[12], (EXPERTS, D, FF), D ** -0.5, 0.125, ((0, 32),))
    w_down = scatter_about(keys[13], (EXPERTS, FF, D), FF ** -0.5, 0.1875, ((0, 32),))
    return dict(pool_input=pool_input, doc_ids=doc_ids, pool_map=pool_map, pool_scale=pool_scale, w_out=w_out, residual=residual, mix_gain=mix_gain, ffn_gain=ffn_gain, out_gain=out_gain, expert_ids=expert_ids, route_logits=route_logits, w_gate=w_gate, w_up=w_up, w_down=w_down)


def rms_scale(vector):
    return lax.rsqrt(lax.optimization_barrier(jnp.mean(vector * vector, axis=-1, keepdims=True)) + 1e-06)

def reference(pool_input, doc_ids, pool_map, pool_scale, w_out, residual, mix_gain, ffn_gain, out_gain, expert_ids, route_logits, w_gate, w_up, w_down):
    total_len = doc_ids.shape[0]
    positions = jnp.arange(total_len, dtype=jnp.int32)
    resets = jnp.concatenate([jnp.ones((1,), bool), doc_ids[1:] != doc_ids[:-1]])
    starts = lax.cummax(jnp.where(resets, positions, 0), axis=0).astype(jnp.int32)
    doc_position = (positions - starts + 1).astype(jnp.int32)
    values = pool_input.astype(jnp.float32)
    prefix = jnp.cumsum(values, axis=2)
    before = jnp.concatenate([jnp.zeros(values.shape[:2] + (1,), jnp.float32), prefix[:, :, :-1]], axis=2)
    running = prefix - jnp.take(before, starts, axis=2)
    mean_list = []
    for group_idx in range(GROUPS):
        span_len = TOK_DEV * 2 ** group_idx
        shifted = jnp.pad(running[group_idx], ((0, 0), (span_len, 0)))[:, :total_len]
        counts_in = jnp.minimum(doc_position, span_len).astype(jnp.float32)
        window = running[group_idx] - jnp.where(doc_position > span_len, shifted, jnp.float32(0.0))
        mean_list.append(window / counts_in)
    window_mean = jnp.stack(mean_list)
    pool_diff = (window_mean - values).astype(jnp.bfloat16)
    mapped = jnp.einsum('gct,gcd->tgd', pool_diff.astype(jnp.float32), pool_map.astype(jnp.float32))
    mapped = (mapped.reshape(total_len, -1) * pool_scale).astype(jnp.bfloat16)
    projected = jnp.dot(mapped, w_out, preferred_element_type=jnp.float32)
    stream = (residual.astype(jnp.float32) + mix_gain * projected * rms_scale(projected)).astype(jnp.bfloat16)
    stream_back = stream.astype(jnp.float32)
    normed = (ffn_gain * stream_back * rms_scale(stream_back)).astype(jnp.bfloat16)
    route_weight = jax.nn.sigmoid(route_logits - route_logits[:, ::-1])
    flat_expert = expert_ids.reshape(-1).astype(jnp.int32)
    flat_weight = route_weight.reshape(-1)
    flat_token = (jnp.arange(flat_expert.shape[0], dtype=jnp.int32) // TOP_K).astype(jnp.int32)
    sort_order = jnp.argsort(flat_expert, stable=True).astype(jnp.int32)
    counts = jnp.bincount(flat_expert, length=EXPERTS).astype(jnp.int32)
    expert_starts = (jnp.cumsum(counts) - counts).astype(jnp.int32)
    most_rows = DEVICES * CAP
    order_padded = jnp.concatenate([sort_order, jnp.zeros((most_rows,), jnp.int32)])

    def one_expert(total_y, expert):
        picked = lax.dynamic_slice_in_dim(order_padded, expert_starts[expert], most_rows)
        live_rows = jnp.arange(most_rows, dtype=jnp.int32) < counts[expert]
        tokens = flat_token[picked]
        row_data = normed[tokens]
        gate_act = jnp.dot(row_data, w_gate[expert], preferred_element_type=jnp.float32)
        up_act = jnp.dot(row_data, w_up[expert], preferred_element_type=jnp.float32)
        hidden = (jax.nn.silu(gate_act) * up_act).astype(jnp.bfloat16)
        expert_out = jnp.dot(hidden, w_down[expert], preferred_element_type=jnp.float32).astype(jnp.bfloat16)
        weight = jnp.where(live_rows, flat_weight[picked], jnp.float32(0.0))
        return (total_y.at[tokens].add(expert_out.astype(jnp.float32) * weight[:, None]), None)
    expert_sum, _ = lax.scan(one_expert, jnp.zeros((total_len, normed.shape[1]), jnp.float32), jnp.arange(EXPERTS, dtype=jnp.int32))
    return (stream_back + out_gain * expert_sum * rms_scale(expert_sum)).astype(jnp.bfloat16)
```

```python
import functools
import jax
import jax.numpy as jnp
from jax import lax
from jax.sharding import PartitionSpec as P
from jax.experimental import pallas as pl
from jax.experimental.pallas import tpu as pltpu

MESH = pl.DeviceIdType.MESH
EPS = 1e-06
CHUNKS = 4
PIECES = 4
F32 = jnp.float32
BF16 = jnp.bfloat16


def rms_scale(vector):
    return lax.rsqrt(jnp.mean(vector * vector, axis=-1, keepdims=True) + EPS)


def contract(left, right, left_dim, right_dim, **options):
    return lax.dot_general(
        left, right, (((left_dim,), (right_dim,)), ((), ())), preferred_element_type=F32, **options
    )


def layer_kernel(
    sp_count, tp_count,
    pool_ref, doc_ref, map_ref, scale_ref, mix_ref, ffn_ref, gain_ref, ids_ref, logits_ref,
    residual_hbm, w_out_hbm, w_gate_hbm, w_up_hbm, w_down_hbm,
    out_ref,
    tail_out, tails, run_out, far, diff_out, parts,
    resid, resid_far, mapped_own, mapped_far, ids_far, logits_far,
    w_out, w_gate, w_up, w_down,
    stream, normed, picked, mix_high, mix_low,
    outgoing, arrived, hidden, finished, results, total, partial_out, partial_in,
    load_sem, tail_send, tail_recv, far_send, far_recv, diff_send, diff_recv,
    mirror_send, mirror_recv, out_send, out_recv, back_send, back_recv, part_send, part_recv,
):
    groups, channels, length = pool_ref.shape
    rows = length // tp_count
    lines = groups * channels
    chunks, _, wide = normed.shape
    peers, capacity = outgoing.shape[2], outgoing.shape[3]
    slots = peers * capacity
    tile, depth = hidden.shape[2], hidden.shape[0]
    sp, tp = lax.axis_index("sp"), lax.axis_index("tp")
    half_count = sp_count // 2
    half = sp // half_count
    me = (sp - half * half_count) * tp_count + tp
    mirror = (lax.rem(sp + half_count, sp_count), tp)

    loads = []
    for i, (source, target) in enumerate((
        (residual_hbm, resid), (w_out_hbm, w_out), (w_gate_hbm.at[0], w_gate),
        (w_up_hbm.at[0], w_up), (w_down_hbm.at[0], w_down),
    )):
        copy = pltpu.make_async_copy(source, target, load_sem.at[i])
        copy.start()
        loads.append(copy)

    barrier = pltpu.get_barrier_semaphore()
    for i in range(1, sp_count):
        pl.semaphore_signal(
            barrier, inc=1, device_id=(lax.rem(sp + i, sp_count), tp), device_id_type=MESH
        )
    for j in range(half_count):
        for i in range(1, tp_count):
            pl.semaphore_signal(
                barrier, inc=1,
                device_id=(half * half_count + j, lax.rem(tp + i, tp_count)),
                device_id_type=MESH,
            )

    values = pool_ref[...].reshape(lines, length)
    doc = doc_ref[...].astype(F32)
    last_id = doc[:, length - 1 :]
    tail_mask = jnp.broadcast_to((doc == last_id).astype(BF16), (8, length))
    tail_sum = contract(tail_mask, values, 1, 1)[:1]
    tail_count = jnp.sum((doc == last_id).astype(F32), axis=1, keepdims=True)
    tail_row = jnp.concatenate(
        [
            tail_sum,
            jnp.broadcast_to(last_id, (1, 128)),
            jnp.broadcast_to(tail_count, (1, 128)),
        ],
        axis=1,
    )
    tail_out[...] = tail_row
    tails[sp] = tail_row
    pl.semaphore_wait(barrier, sp_count - 1 + half_count * (tp_count - 1))
    tail_copies = []
    for i in range(1, sp_count):
        copy = pltpu.make_async_remote_copy(
            src_ref=tail_out,
            dst_ref=tails.at[sp],
            send_sem=tail_send.at[i],
            recv_sem=tail_recv.at[i],
            device_id=(lax.rem(sp + i, sp_count), tp),
            device_id_type=MESH,
        )
        copy.start()
        tail_copies.append(copy)

    mirror_copies = []

    def to_mirror(source, target):
        i = len(mirror_copies)
        copy = pltpu.make_async_remote_copy(
            src_ref=source,
            dst_ref=target,
            send_sem=mirror_send.at[i],
            recv_sem=mirror_recv.at[i],
            device_id=mirror,
            device_id_type=MESH,
        )
        copy.start()
        mirror_copies.append(copy)

    to_mirror(ids_ref, ids_far)
    to_mirror(logits_ref, logits_far)
    loads[0].wait()
    piece = rows // PIECES
    to_mirror(resid.at[pl.ds(0, piece)], resid_far.at[pl.ds(0, piece)])

    doc_col = jnp.broadcast_to(doc, (128, length)).T[:, :1]
    row_at = lax.broadcasted_iota(jnp.int32, (length, length), 0)
    col_at = lax.broadcasted_iota(jnp.int32, (length, length), 1)
    same = jnp.where((row_at <= col_at) & (doc_col == doc), 1.0, 0.0)
    local_count = jnp.sum(same, axis=0, keepdims=True)
    local_run = jnp.dot(values, same.astype(BF16), preferred_element_type=F32)

    for copy in tail_copies:
        copy.wait()
    table = jnp.concatenate([tails[j] for j in range(sp_count)], axis=0)
    sources = lax.broadcasted_iota(jnp.int32, (sp_count, 1), 0)
    joined = jnp.where((sources < sp) & (table[:, lines : lines + 1] == doc), 1.0, 0.0)
    running = local_run + contract(
        table[:, :lines], joined, 0, 0, precision=lax.Precision.HIGHEST
    )
    position = local_count + jnp.sum(
        joined * table[:, lines + 128 : lines + 129], axis=0, keepdims=True
    )
    run_out[...] = running.astype(BF16).reshape(groups, channels, length)
    far_copies = []
    for g in reversed(range(groups)):
        copy = pltpu.make_async_remote_copy(
            src_ref=run_out.at[g],
            dst_ref=far.at[g],
            send_sem=far_send.at[g],
            recv_sem=far_recv.at[g],
            device_id=(lax.rem(sp + 2**g, sp_count), tp),
            device_id_type=MESH,
        )
        copy.start()
        far_copies.append(copy)
    for i in range(1, PIECES):
        at = pl.ds(i * piece, piece)
        to_mirror(resid.at[at], resid_far.at[at])

    expand = (
        lax.broadcasted_iota(jnp.int32, (slots, peers), 0) // capacity
        == lax.broadcasted_iota(jnp.int32, (slots, peers), 1)
    ).astype(BF16)
    at_row = lax.broadcasted_iota(jnp.int32, (rows, rows), 0)
    at_col = lax.broadcasted_iota(jnp.int32, (rows, rows), 1)
    earlier = (at_row < at_col).astype(BF16)
    slot_down = lax.rem(lax.broadcasted_iota(jnp.int32, (slots, rows), 0), capacity).astype(F32)
    slot_across = lax.rem(lax.broadcasted_iota(jnp.int32, (rows, slots), 1), capacity).astype(F32)
    experts = lax.broadcasted_iota(jnp.int32, (peers, rows), 0) + half * peers

    def place(block, ids, logits):
        first, second = ids[0:1] == experts, ids[1:2] == experts
        named = jnp.where(first | second, 1.0, 0.0)
        rank = jnp.dot(named.astype(BF16), earlier, preferred_element_type=F32)
        code = jnp.where(named > 0.0, rank, -1.0).astype(BF16)
        picked[block] = jnp.where(
            jnp.dot(expand, code, preferred_element_type=F32) == slot_down, 1.0, 0.0
        ).astype(BF16)
        weight = jnp.where(first, jax.nn.sigmoid(logits[0:1] - logits[1:2]), 0.0) + jnp.where(
            second, jax.nn.sigmoid(logits[1:2] - logits[0:1]), 0.0
        )
        high = weight.astype(BF16)
        low = (weight - high.astype(F32)).astype(BF16)
        here = contract(code, expand, 0, 1) == slot_across
        mix_high[block] = jnp.where(here, contract(high, expand, 0, 1), 0.0).astype(BF16)
        mix_low[block] = jnp.where(here, contract(low, expand, 0, 1), 0.0).astype(BF16)

    place(0, ids_ref[...], logits_ref[...])

    for copy in far_copies:
        copy.wait()
    for g in range(groups):
        span = float(length * 2**g)
        at = slice(g * channels, (g + 1) * channels)
        window = running[at] - jnp.where(position > span, far[g].astype(F32), 0.0)
        diff = window / jnp.minimum(position, span) - values[at].astype(F32)
        diff = diff.astype(BF16)
        for q in range(tp_count):
            diff_out[q, g] = diff[:, q * rows : (q + 1) * rows]
    parts[tp] = diff_out[tp]
    diff_copies = []
    for i in range(1, tp_count):
        other = lax.rem(tp + i, tp_count)
        copy = pltpu.make_async_remote_copy(
            src_ref=diff_out.at[other],
            dst_ref=parts.at[tp],
            send_sem=diff_send.at[i],
            recv_sem=diff_recv.at[i],
            device_id=(sp, other),
            device_id_type=MESH,
        )
        copy.start()
        diff_copies.append(copy)
    for copy in diff_copies:
        copy.wait()
    for g in range(groups):
        channel_rows = jnp.concatenate([parts[q, g] for q in range(tp_count)], axis=0)
        size = tp_count * channels
        at = slice(g * size, (g + 1) * size)
        mapped_own[:, at] = (contract(channel_rows, map_ref[g], 0, 0) * scale_ref[:, at]).astype(BF16)
    to_mirror(mapped_own, mapped_far)
    loads[1].wait()

    step = min(rows, 128)

    def norm_rows(mapped_ref, resid_ref, keep):
        def body(i, carry):
            at = pl.ds(pl.multiple_of(i * step, step), step)
            projected = jnp.dot(mapped_ref[at, :], w_out[...], preferred_element_type=F32)
            line = (
                resid_ref[at, :].astype(F32) + mix_ref[...] * projected * rms_scale(projected)
            ).astype(BF16)
            if keep:
                stream[at, :] = line
            back = line.astype(F32)
            ready = (ffn_ref[...] * back * rms_scale(back)).astype(BF16)
            for c in range(chunks):
                normed[c, at, :] = ready[:, c * wide : (c + 1) * wide]
            return carry

        lax.fori_loop(0, rows // step, body, 0)

    def spread(source, target, send, recv, block, c):
        def body(i, carry):
            peer = lax.rem(me + i, peers)
            place_sp = half * half_count + peer // tp_count
            pltpu.make_async_remote_copy(
                src_ref=source.at[block, c, peer],
                dst_ref=target.at[block, c, me],
                send_sem=send.at[block, c],
                recv_sem=recv.at[block, c],
                device_id=(place_sp, lax.rem(peer, tp_count)),
                device_id_type=MESH,
            ).start()
            return carry

        lax.fori_loop(1, peers, body, 0)
        target[block, c, me] = source[block, c, me]

    def settle(buffer, sem, block, c):
        whole = buffer.at[block, c, pl.ds(0, peers - 1)]
        pltpu.make_async_copy(whole, whole, sem.at[block, c]).wait()

    def hand_out(block):
        def body(c, carry):
            packed = jnp.dot(picked[block], normed[c], preferred_element_type=F32)
            outgoing[block, c] = packed.astype(BF16).reshape(peers, capacity, wide)
            spread(outgoing, arrived, out_send, out_recv, block, c)
            return carry

        lax.fori_loop(0, chunks, body, 0)

    def expert_in(block):
        def body(f, carry):
            at = pl.ds(pl.multiple_of(f * tile, tile), tile)
            gate = jnp.zeros((slots, tile), F32)
            up = jnp.zeros((slots, tile), F32)
            for c in range(chunks):
                line = arrived[block, c].reshape(slots, wide)
                inner = slice(c * wide, (c + 1) * wide)
                gate = gate + jnp.dot(line, w_gate[inner, at], preferred_element_type=F32)
                up = up + jnp.dot(line, w_up[inner, at], preferred_element_type=F32)
            hidden[f] = (jax.nn.silu(gate) * up).astype(BF16)
            return carry

        lax.fori_loop(0, depth, body, 0)

    def expert_out(block, then):
        def body(c, carry):
            at = pl.ds(pl.multiple_of(c * wide, wide), wide)
            value = jnp.zeros((slots, wide), F32)
            for f in range(depth):
                inner = slice(f * tile, (f + 1) * tile)
                value = value + jnp.dot(hidden[f], w_down[inner, at], preferred_element_type=F32)
            finished[block, c] = value.astype(BF16).reshape(peers, capacity, wide)
            if then:
                spread(finished, results, back_send, back_recv, block, c)
            return carry

        lax.fori_loop(0, chunks, body, 0)

    def gathered(block, c):
        line = results[block, c].reshape(slots, wide)
        return jnp.dot(mix_high[block], line, preferred_element_type=F32) + jnp.dot(
            mix_low[block], line, preferred_element_type=F32
        )

    norm_rows(mapped_own, resid, True)
    hand_out(0)
    for copy in mirror_copies[:2]:
        copy.wait()
    place(1, ids_far[...], logits_far[...])
    for copy in mirror_copies[2:]:
        copy.wait()
    norm_rows(mapped_far, resid_far, False)
    hand_out(1)

    for copy in loads[2:]:
        copy.wait()
    for c in range(chunks):
        settle(arrived, out_recv, 0, c)
    expert_in(0)
    expert_out(0, False)
    for c in range(chunks):
        settle(arrived, out_recv, 1, c)
    expert_in(1)
    expert_out(1, True)
    for c in range(chunks):
        spread(finished, results, back_send, back_recv, 0, c)
    part_copies = []
    for c in range(chunks):
        settle(results, back_recv, 1, c)
        partial_out[c] = gathered(1, c).astype(BF16)
        copy = pltpu.make_async_remote_copy(
            src_ref=partial_out.at[c],
            dst_ref=partial_in.at[c],
            send_sem=part_send.at[c],
            recv_sem=part_recv.at[c],
            device_id=mirror,
            device_id_type=MESH,
        )
        copy.start()
        part_copies.append(copy)
    for c in range(chunks):
        settle(results, back_recv, 0, c)
        total[c] = gathered(0, c)
    for block in range(2):
        for c in range(chunks):
            settle(outgoing, out_send, block, c)
            settle(finished, back_send, block, c)
    for copy in part_copies:
        copy.wait()

    def finish(i, carry):
        at = pl.ds(pl.multiple_of(i * step, step), step)
        summed = jnp.concatenate(
            [total[c, at, :] + partial_in[c, at, :].astype(F32) for c in range(chunks)], axis=1
        )
        out_ref[at, :] = (
            stream[at, :].astype(F32) + gain_ref[...] * summed * rms_scale(summed)
        ).astype(BF16)
        return carry

    lax.fori_loop(0, rows // step, finish, 0)


def local(
    pool_input, doc_ids, pool_map, pool_scale, w_out, residual, mix_gain, ffn_gain, out_gain,
    expert_ids, route_logits, w_gate, w_up, w_down,
):
    groups, channels, length = pool_input.shape
    sp_count, tp_count = lax.axis_size("sp"), lax.axis_size("tp")
    rows, top_count = expert_ids.shape
    width, hidden_width = w_gate.shape[1], w_gate.shape[2]
    experts = sp_count * tp_count
    peers = experts // 2
    capacity = max(16, 2 * rows * top_count // experts)
    slots = peers * capacity
    pool_width = w_out.shape[0]
    wide, tile = width // CHUNKS, 256
    tail_width = groups * channels + 256
    vmem = pl.BlockSpec(memory_space=pltpu.VMEM)
    hbm = pl.BlockSpec(memory_space=pl.ANY)
    exchange = pltpu.VMEM((2, CHUNKS, peers, capacity, wide), BF16)
    dma = pltpu.SemaphoreType.DMA
    return pl.pallas_call(
        functools.partial(layer_kernel, sp_count, tp_count),
        out_shape=jax.ShapeDtypeStruct(residual.shape, BF16),
        in_specs=[vmem] * 9 + [hbm] * 5,
        out_specs=vmem,
        scratch_shapes=[
            pltpu.VMEM((1, tail_width), F32),
            pltpu.VMEM((sp_count, 1, tail_width), F32),
            pltpu.VMEM((groups, channels, length), BF16),
            pltpu.VMEM((groups, channels, length), BF16),
            pltpu.VMEM((tp_count, groups, channels, rows), BF16),
            pltpu.VMEM((tp_count, groups, channels, rows), BF16),
            pltpu.VMEM((rows, width), BF16),
            pltpu.VMEM((rows, width), BF16),
            pltpu.VMEM((rows, pool_width), BF16),
            pltpu.VMEM((rows, pool_width), BF16),
            pltpu.VMEM((top_count, rows), jnp.int32),
            pltpu.VMEM((top_count, rows), F32),
            pltpu.VMEM((pool_width, width), BF16),
            pltpu.VMEM((width, hidden_width), BF16),
            pltpu.VMEM((width, hidden_width), BF16),
            pltpu.VMEM((hidden_width, width), BF16),
            pltpu.VMEM((rows, width), BF16),
            pltpu.VMEM((CHUNKS, rows, wide), BF16),
            pltpu.VMEM((2, slots, rows), BF16),
            pltpu.VMEM((2, rows, slots), BF16),
            pltpu.VMEM((2, rows, slots), BF16),
            exchange,
            exchange,
            pltpu.VMEM((hidden_width // tile, slots, tile), BF16),
            exchange,
            exchange,
            pltpu.VMEM((CHUNKS, rows, wide), F32),
            pltpu.VMEM((CHUNKS, rows, wide), BF16),
            pltpu.VMEM((CHUNKS, rows, wide), BF16),
            dma((5,)),
            dma((sp_count,)),
            dma((sp_count,)),
            dma((groups,)),
            dma((groups,)),
            dma((tp_count,)),
            dma((tp_count,)),
            dma((PIECES + 3,)),
            dma((PIECES + 3,)),
            dma((2, CHUNKS)),
            dma((2, CHUNKS)),
            dma((2, CHUNKS)),
            dma((2, CHUNKS)),
            dma((CHUNKS,)),
            dma((CHUNKS,)),
        ],
        compiler_params=pltpu.CompilerParams(
            collective_id=0, has_side_effects=True, vmem_limit_bytes=67043328
        ),
    )(
        pool_input,
        doc_ids.reshape(1, -1),
        pool_map,
        pool_scale.reshape(1, -1),
        mix_gain.reshape(1, -1),
        ffn_gain.reshape(1, -1),
        out_gain.reshape(1, -1),
        expert_ids.T,
        route_logits.T,
        residual,
        w_out,
        w_gate,
        w_up,
        w_down,
    )


def solution(mesh):
    rows = P(("sp", "tp"), None)
    cubes = P(("sp", "tp"), None, None)
    in_specs = (
        P(None, "tp", "sp"), P("sp"), P(), P(), P(), rows, P(), P(), P(), rows, rows,
        cubes, cubes, cubes,
    )
    return jax.shard_map(local, mesh=mesh, in_specs=in_specs, out_specs=rows, check_vma=False)
```

```python
import functools
import jax
import jax.numpy as jnp
from jax import lax
from jax.sharding import PartitionSpec as P
from jax.experimental import pallas as pl
from jax.experimental.pallas import tpu as pltpu

MESH = pl.DeviceIdType.MESH
EPS = 1e-06
CHUNKS = 4
PLANES = 4
F32 = jnp.float32
BF16 = jnp.bfloat16


def rms_scale(vector):
    return lax.rsqrt(jnp.mean(vector * vector, axis=-1, keepdims=True) + EPS)


def contract(left, right, left_dim, right_dim, **options):
    return lax.dot_general(
        left, right, (((left_dim,), (right_dim,)), ((), ())), preferred_element_type=F32, **options
    )


VISITS = ((0, 1, 2, 3), (1, 0, 2, 3), (2, 3, 1, 0), (3, 2, 1, 0))


def layer_kernel(
    sp_count, tp_count,
    pool_ref, doc_ref, map_ref, scale_ref, mix_ref, ffn_ref, gain_ref, ids_ref, logits_ref,
    residual_hbm, w_out_hbm, w_gate_hbm, w_up_hbm, w_down_hbm,
    out_ref,
    tail_out, tails, run_out, far, diff_out, parts, route_own, routes,
    resid, mapped, w_out, w_gate, w_up, w_down,
    stream, normed, picked, mix_high, mix_low,
    outgoing, arrived, hidden, finished, results, total, partial_out, partial_in,
    load_sem, tail_send, tail_recv, far_send, far_recv, diff_send, diff_recv,
    route_send, route_recv, up_send, down_send, line_recv,
    out_send, out_recv, back_send, back_recv, part_send, part_recv,
):
    groups, channels, length = pool_ref.shape
    rows = length // tp_count
    lines = groups * channels
    chunks, wide = normed.shape[1], normed.shape[3]
    peers, capacity = outgoing.shape[2], outgoing.shape[3]
    slots = peers * capacity
    depth, _, tile = hidden.shape
    sp, tp = lax.axis_index("sp"), lax.axis_index("tp")
    plane_size = sp_count // PLANES
    plane = sp // plane_size
    spot = sp - plane * plane_size
    me = spot * tp_count + tp
    last = PLANES - 1
    low, high = plane == 0, plane == last
    visits = [
        sum((plane == q).astype(jnp.int32) * s for q, s in enumerate(column))
        for column in zip(*VISITS)
    ]

    def in_line(other):
        return (other * plane_size + spot, tp)

    loads = []
    for i, (source, target) in enumerate((
        (residual_hbm, resid), (w_out_hbm, w_out), (w_gate_hbm.at[0], w_gate),
        (w_up_hbm.at[0], w_up), (w_down_hbm.at[0], w_down),
    )):
        copy = pltpu.make_async_copy(source, target, load_sem.at[i])
        copy.start()
        loads.append(copy)

    barrier = pltpu.get_barrier_semaphore()
    for i in range(1, sp_count):
        pl.semaphore_signal(
            barrier, inc=1, device_id=(lax.rem(sp + i, sp_count), tp), device_id_type=MESH
        )
    for j in range(plane_size):
        for i in range(1, tp_count):
            pl.semaphore_signal(
                barrier, inc=1,
                device_id=(plane * plane_size + j, lax.rem(tp + i, tp_count)),
                device_id_type=MESH,
            )

    values = pool_ref[...].reshape(lines, length)
    doc = doc_ref[...].astype(F32)
    last_id = doc[:, length - 1 :]
    tail_mask = jnp.broadcast_to((doc == last_id).astype(BF16), (8, length))
    tail_sum = contract(tail_mask, values, 1, 1)[:1]
    tail_count = jnp.sum((doc == last_id).astype(F32), axis=1, keepdims=True)
    tail_row = jnp.concatenate(
        [
            tail_sum,
            jnp.broadcast_to(last_id, (1, 128)),
            jnp.broadcast_to(tail_count, (1, 128)),
        ],
        axis=1,
    )
    tail_out[...] = tail_row
    tails[sp] = tail_row
    route = jnp.concatenate([ids_ref[...].astype(F32), logits_ref[...]], axis=0)
    route_own[...] = route
    routes[plane] = route
    doc_col = jnp.broadcast_to(doc, (128, length)).T[:, :1]
    row_at = lax.broadcasted_iota(jnp.int32, (length, length), 0)
    col_at = lax.broadcasted_iota(jnp.int32, (length, length), 1)
    same = jnp.where((row_at <= col_at) & (doc_col == doc), 1.0, 0.0)
    local_count = jnp.sum(same, axis=0, keepdims=True)
    local_run = jnp.dot(values, same.astype(BF16), preferred_element_type=F32)
    run_out[...] = local_run.astype(BF16).reshape(groups, channels, length)
    pl.semaphore_wait(barrier, sp_count - 1 + plane_size * (tp_count - 1))

    def send(source, target, send_sem, recv_sem, device):
        copy = pltpu.make_async_remote_copy(
            src_ref=source,
            dst_ref=target,
            send_sem=send_sem,
            recv_sem=recv_sem,
            device_id=device,
            device_id_type=MESH,
        )
        copy.start()
        return copy

    early = [
        send(
            tail_out, tails.at[sp], tail_send.at[i], tail_recv.at[i],
            (lax.rem(sp + i, sp_count), tp),
        )
        for i in range(1, sp_count)
    ]
    early += [
        send(
            run_out.at[g], far.at[g], far_send.at[g], far_recv.at[g],
            (lax.rem(sp + 2**g, sp_count), tp),
        )
        for g in reversed(range(groups))
    ]
    route_copies = [
        send(
            route_own, routes.at[plane], route_send.at[i], route_recv.at[i],
            in_line(lax.rem(plane + i, PLANES)),
        )
        for i in range(1, PLANES)
    ]

    expand = (
        lax.broadcasted_iota(jnp.int32, (slots, peers), 0) // capacity
        == lax.broadcasted_iota(jnp.int32, (slots, peers), 1)
    ).astype(BF16)
    at_row = lax.broadcasted_iota(jnp.int32, (rows, rows), 0)
    at_col = lax.broadcasted_iota(jnp.int32, (rows, rows), 1)
    earlier = (at_row < at_col).astype(BF16)
    slot_down = lax.rem(lax.broadcasted_iota(jnp.int32, (slots, rows), 0), capacity).astype(F32)
    slot_across = lax.rem(lax.broadcasted_iota(jnp.int32, (rows, slots), 1), capacity).astype(F32)
    experts = (lax.broadcasted_iota(jnp.int32, (peers, rows), 0) + plane * peers).astype(F32)

    def place(block):
        route = routes[block]
        first, second = route[0:1] == experts, route[1:2] == experts
        named = jnp.where(first | second, 1.0, 0.0)
        rank = jnp.dot(named.astype(BF16), earlier, preferred_element_type=F32)
        code = jnp.where(named > 0.0, rank, -1.0).astype(BF16)
        picked[block] = jnp.where(
            jnp.dot(expand, code, preferred_element_type=F32) == slot_down, 1.0, 0.0
        ).astype(BF16)
        weight = jnp.where(first, jax.nn.sigmoid(route[2:3] - route[3:4]), 0.0) + jnp.where(
            second, jax.nn.sigmoid(route[3:4] - route[2:3]), 0.0
        )
        top = weight.astype(BF16)
        rest = (weight - top.astype(F32)).astype(BF16)
        here = contract(code, expand, 0, 1) == slot_across
        mix_high[block] = jnp.where(here, contract(top, expand, 0, 1), 0.0).astype(BF16)
        mix_low[block] = jnp.where(here, contract(rest, expand, 0, 1), 0.0).astype(BF16)

    for copy in early:
        copy.wait()
    table = jnp.concatenate([tails[j] for j in range(sp_count)], axis=0)
    sources = lax.broadcasted_iota(jnp.int32, (sp_count, 1), 0)
    joined = jnp.where((sources < sp) & (table[:, lines : lines + 1] == doc), 1.0, 0.0)
    position = local_count + jnp.sum(
        joined * table[:, lines + 128 : lines + 129], axis=0, keepdims=True
    )
    for g in range(groups):
        span = float(length * 2**g)
        at = slice(g * channels, (g + 1) * channels)
        between = contract(
            table[:, at], jnp.where(sources >= sp - 2**g, joined, 0.0), 0, 0,
            precision=lax.Precision.HIGHEST,
        )
        window = local_run[at] + between - jnp.where(position > span, far[g].astype(F32), 0.0)
        diff = window / jnp.minimum(position, span) - values[at].astype(F32)
        diff = diff.astype(BF16)
        for q in range(tp_count):
            diff_out[q, g] = diff[:, q * rows : (q + 1) * rows]
    parts[tp] = diff_out[tp]
    diff_copies = []
    for i in range(1, tp_count):
        other = lax.rem(tp + i, tp_count)
        diff_copies.append(
            send(diff_out.at[other], parts.at[tp], diff_send.at[i], diff_recv.at[i], (sp, other))
        )
    place(plane)
    loads[0].wait()
    loads[1].wait()
    for copy in diff_copies:
        copy.wait()
    for g in range(groups):
        channel_rows = jnp.concatenate([parts[q, g] for q in range(tp_count)], axis=0)
        size = tp_count * channels
        at = slice(g * size, (g + 1) * size)
        mapped[:, at] = (contract(channel_rows, map_ref[g], 0, 0) * scale_ref[:, at]).astype(BF16)

    step = min(rows, 128)

    def norm_rows(i, carry):
        at = pl.ds(pl.multiple_of(i * step, step), step)
        projected = jnp.dot(mapped[at, :], w_out[...], preferred_element_type=F32)
        line = (
            resid[at, :].astype(F32) + mix_ref[...] * projected * rms_scale(projected)
        ).astype(BF16)
        stream[at, :] = line
        back = line.astype(F32)
        ready = (ffn_ref[...] * back * rms_scale(back)).astype(BF16)
        for c in range(chunks):
            normed[plane, c, at, :] = ready[:, c * wide : (c + 1) * wide]
        return carry

    lax.fori_loop(0, rows // step, norm_rows, 0)

    def pass_on(s, c, upward, wait):
        target = plane + 1 if upward else plane - 1
        copy = pltpu.make_async_remote_copy(
            src_ref=normed.at[s, c],
            dst_ref=normed.at[s, c],
            send_sem=(up_send if upward else down_send).at[s, c],
            recv_sem=line_recv.at[s, c],
            device_id=in_line(target),
            device_id_type=MESH,
        )
        if wait:
            copy.wait_send()
        else:
            copy.start()

    def pass_both(s, c, wait=False):
        @pl.when((s <= plane) & (plane < last))
        def _():
            pass_on(s, c, True, wait)

        @pl.when((s >= plane) & (plane > 0))
        def _():
            pass_on(s, c, False, wait)

    def spread(source, target, send_sem, recv_sem, k, c):
        def body(i, carry):
            peer = lax.rem(me + i, peers)
            pltpu.make_async_remote_copy(
                src_ref=source.at[k, c, peer],
                dst_ref=target.at[k, c, me],
                send_sem=send_sem.at[k, c],
                recv_sem=recv_sem.at[k, c],
                device_id=(plane * plane_size + peer // tp_count, lax.rem(peer, tp_count)),
                device_id_type=MESH,
            ).start()
            return carry

        lax.fori_loop(1, peers, body, 0)
        target[k, c, me] = source[k, c, me]

    def settle(buffer, sem, k, c):
        whole = buffer.at[k, c, pl.ds(0, peers - 1)]
        pltpu.make_async_copy(whole, whole, sem.at[k, c]).wait()

    def every(body, first=0, end=4):
        def wrapped(c, carry):
            body(c)
            return carry

        lax.fori_loop(chunks * first // 4, chunks * end // 4, wrapped, 0)

    def hand_out(k, c):
        s = visits[k]
        if k > 0:
            pltpu.make_async_copy(normed.at[s, c], normed.at[s, c], line_recv.at[s, c]).wait()
            pass_both(s, c)
        packed = jnp.dot(picked[s], normed[s, c], preferred_element_type=F32)
        outgoing[k, c] = packed.astype(BF16).reshape(peers, capacity, wide)
        spread(outgoing, arrived, out_send, out_recv, k, c)

    def give_out(k, c):
        spread(finished, results, back_send, back_recv, k, c)

    def run_expert(k, give):
        every(lambda c: settle(arrived, out_recv, k, c))

        def body(f, carry):
            at = pl.ds(pl.multiple_of(f * tile, tile), tile)
            gate = jnp.zeros((slots, tile), F32)
            up = jnp.zeros((slots, tile), F32)
            for c in range(chunks):
                line = arrived[k, c].reshape(slots, wide)
                inner = slice(c * wide, (c + 1) * wide)
                gate = gate + jnp.dot(line, w_gate[inner, at], preferred_element_type=F32)
                up = up + jnp.dot(line, w_up[inner, at], preferred_element_type=F32)
            hidden[f] = (jax.nn.silu(gate) * up).astype(BF16)
            return carry

        lax.fori_loop(0, depth, body, 0)

        def give_back(c):
            at = pl.ds(pl.multiple_of(c * wide, wide), wide)
            value = jnp.zeros((slots, wide), F32)
            for f in range(depth):
                inner = slice(f * tile, (f + 1) * tile)
                value = value + jnp.dot(hidden[f], w_down[inner, at], preferred_element_type=F32)
            finished[k, c] = value.astype(BF16).reshape(peers, capacity, wide)
            if give:
                give_out(k, c)

        every(give_back)

    def gathered(k, c):
        s = visits[k]
        settle(results, back_recv, k, c)
        line = results[k, c].reshape(slots, wide)
        return jnp.dot(mix_high[s], line, preferred_element_type=F32) + jnp.dot(
            mix_low[s], line, preferred_element_type=F32
        )

    def part_copy(k, c):
        s = visits[k]
        target = jnp.where(s > plane, plane + 1, plane - 1)
        slot = jnp.where(s == plane - 1, PLANES, s)
        return pltpu.make_async_remote_copy(
            src_ref=partial_out.at[s, c],
            dst_ref=partial_in.at[slot, c],
            send_sem=part_send.at[s, c],
            recv_sem=part_recv.at[slot, c],
            device_id=in_line(target),
            device_id_type=MESH,
        )

    def await_part(slot, c):
        ref = partial_in.at[slot, c]
        pltpu.make_async_copy(ref, ref, part_recv.at[slot, c]).wait()

    def give_end(k, c):
        partial_out[visits[k], c] = gathered(k, c).astype(BF16)
        part_copy(k, c).start()

    def give_middle(k, c):
        s = visits[k]
        value = gathered(k, c)
        await_part(s, c)
        partial_out[s, c] = (value + partial_in[s, c].astype(F32)).astype(BF16)
        part_copy(k, c).start()

    def hand(k, first=0, end=4):
        every(lambda c: hand_out(k, c), first, end)

    def part(k, first=0, end=4):
        every(lambda c: give_end(k, c), first, end)

    def own(c):
        total[c] = gathered(0, c)

    every(lambda c: pass_both(plane, c))
    hand(0)
    for copy in route_copies:
        copy.wait()
    for k in range(1, PLANES):
        place(visits[k])
    for copy in loads[2:]:
        copy.wait()

    @pl.when(low | high)
    def _():
        hand(1)
        run_expert(0, False)
        run_expert(1, True)
        hand(2, 0, 2)
        part(1, 0, 2)
        hand(2, 2, 3)
        part(1, 2, 3)
        hand(2, 3, 4)
        part(1, 3, 4)
        run_expert(2, True)
        hand(3, 0, 2)
        part(2, 0, 2)
        hand(3, 2, 3)
        part(2, 2, 3)
        hand(3, 3, 4)
        part(2, 3, 4)
        run_expert(3, True)
        every(lambda c: give_out(0, c))
        part(3)
        every(own)

    @pl.when(jnp.logical_not(low | high))
    def _():
        def both_in(c):
            hand_out(1, c)
            hand_out(2, c)

        every(both_in)
        run_expert(0, False)
        hand(3, 0, 1)
        run_expert(1, False)
        hand(3, 1, 2)
        run_expert(2, True)
        hand(3, 2, 4)
        every(lambda c: give_out(1, c))
        run_expert(3, True)
        every(lambda c: give_out(0, c))
        every(lambda c: give_middle(2, c))

        def both_out(c):
            give_middle(3, c)
            give_middle(1, c)

        every(both_out)
        every(own)

    @pl.when(plane > 0)
    def _():
        def body(c):
            await_part(plane, c)
            total[c] = total[c] + partial_in[plane, c].astype(F32)

        every(body)

    @pl.when(plane < last)
    def _():
        def body(c):
            await_part(PLANES, c)
            total[c] = total[c] + partial_in[PLANES, c].astype(F32)

        every(body)

    def finish(i, carry):
        at = pl.ds(pl.multiple_of(i * step, step), step)
        summed = jnp.concatenate([total[c, at, :] for c in range(chunks)], axis=1)
        out_ref[at, :] = (
            stream[at, :].astype(F32) + gain_ref[...] * summed * rms_scale(summed)
        ).astype(BF16)
        return carry

    lax.fori_loop(0, rows // step, finish, 0)
    for k in range(PLANES):
        every(lambda c: settle(outgoing, out_send, k, c))
        every(lambda c: settle(finished, back_send, k, c))
        every(lambda c: pass_both(visits[k], c, True))
        if k > 0:
            every(lambda c: part_copy(k, c).wait_send())


def local(
    pool_input, doc_ids, pool_map, pool_scale, w_out, residual, mix_gain, ffn_gain, out_gain,
    expert_ids, route_logits, w_gate, w_up, w_down,
):
    groups, channels, length = pool_input.shape
    sp_count, tp_count = lax.axis_size("sp"), lax.axis_size("tp")
    rows, top_count = expert_ids.shape
    width, hidden_width = w_gate.shape[1], w_gate.shape[2]
    experts = sp_count * tp_count
    peers = experts // PLANES
    capacity = max(16, 2 * rows * top_count // experts)
    slots = peers * capacity
    pool_width = w_out.shape[0]
    wide, tile = width // CHUNKS, 256
    tail_width = groups * channels + 256
    vmem = pl.BlockSpec(memory_space=pltpu.VMEM)
    hbm = pl.BlockSpec(memory_space=pl.ANY)
    exchange = pltpu.VMEM((PLANES, CHUNKS, peers, capacity, wide), BF16)
    dma = pltpu.SemaphoreType.DMA
    each = dma((PLANES, CHUNKS))
    return pl.pallas_call(
        functools.partial(layer_kernel, sp_count, tp_count),
        out_shape=jax.ShapeDtypeStruct(residual.shape, BF16),
        in_specs=[vmem] * 9 + [hbm] * 5,
        out_specs=vmem,
        scratch_shapes=[
            pltpu.VMEM((1, tail_width), F32),
            pltpu.VMEM((sp_count, 1, tail_width), F32),
            pltpu.VMEM((groups, channels, length), BF16),
            pltpu.VMEM((groups, channels, length), BF16),
            pltpu.VMEM((tp_count, groups, channels, rows), BF16),
            pltpu.VMEM((tp_count, groups, channels, rows), BF16),
            pltpu.VMEM((2 * top_count, rows), F32),
            pltpu.VMEM((PLANES, 2 * top_count, rows), F32),
            pltpu.VMEM((rows, width), BF16),
            pltpu.VMEM((rows, pool_width), BF16),
            pltpu.VMEM((pool_width, width), BF16),
            pltpu.VMEM((width, hidden_width), BF16),
            pltpu.VMEM((width, hidden_width), BF16),
            pltpu.VMEM((hidden_width, width), BF16),
            pltpu.VMEM((rows, width), BF16),
            pltpu.VMEM((PLANES, CHUNKS, rows, wide), BF16),
            pltpu.VMEM((PLANES, slots, rows), BF16),
            pltpu.VMEM((PLANES, rows, slots), BF16),
            pltpu.VMEM((PLANES, rows, slots), BF16),
            exchange,
            exchange,
            pltpu.VMEM((hidden_width // tile, slots, tile), BF16),
            exchange,
            exchange,
            pltpu.VMEM((CHUNKS, rows, wide), F32),
            pltpu.VMEM((PLANES, CHUNKS, rows, wide), BF16),
            pltpu.VMEM((PLANES + 1, CHUNKS, rows, wide), BF16),
            dma((5,)),
            dma((sp_count,)),
            dma((sp_count,)),
            dma((groups,)),
            dma((groups,)),
            dma((tp_count,)),
            dma((tp_count,)),
            dma((PLANES,)),
            dma((PLANES,)),
            each,
            each,
            each,
            each,
            each,
            each,
            each,
            each,
            dma((PLANES + 1, CHUNKS)),
        ],
        compiler_params=pltpu.CompilerParams(
            collective_id=0, has_side_effects=True, vmem_limit_bytes=67043328
        ),
    )(
        pool_input,
        doc_ids.reshape(1, -1),
        pool_map,
        pool_scale.reshape(1, -1),
        mix_gain.reshape(1, -1),
        ffn_gain.reshape(1, -1),
        out_gain.reshape(1, -1),
        expert_ids.T,
        route_logits.T,
        residual,
        w_out,
        w_gate,
        w_up,
        w_down,
    )


def solution(mesh):
    rows = P(("sp", "tp"), None)
    cubes = P(("sp", "tp"), None, None)
    in_specs = (
        P(None, "tp", "sp"), P("sp"), P(), P(), P(), rows, P(), P(), P(), rows, rows,
        cubes, cubes, cubes,
    )
    return jax.shard_map(local, mesh=mesh, in_specs=in_specs, out_specs=rows, check_vma=False)
```

```python
import functools
import jax
import jax.numpy as jnp
from jax import lax
from jax.sharding import PartitionSpec as P
from jax.experimental import pallas as pl
from jax.experimental.pallas import tpu as pltpu

MESH = pl.DeviceIdType.MESH
EPS = 1e-06
CHUNKS = 4
PLANES = 4
F32 = jnp.float32
BF16 = jnp.bfloat16


def rms_scale(vector):
    return lax.rsqrt(jnp.mean(vector * vector, axis=-1, keepdims=True) + EPS)


def contract(left, right, left_dim, right_dim, **options):
    return lax.dot_general(
        left, right, (((left_dim,), (right_dim,)), ((), ())), preferred_element_type=F32, **options
    )


VISITS = ((0, 2, 3, 1), (1, 0, 2, 3), (2, 3, 1, 0), (3, 1, 0, 2))


def remote(source, target, send_sem, recv_sem, device):
    return pltpu.make_async_remote_copy(
        src_ref=source,
        dst_ref=target,
        send_sem=send_sem,
        recv_sem=recv_sem,
        device_id=device,
        device_id_type=MESH,
    )


def send(*copy):
    made = remote(*copy)
    made.start()
    return made


def mixer_kernel(
    sp_count, tp_count,
    pool_ref, doc_ref, map_ref, scale_ref, mix_ref, ffn_ref, ids_ref, logits_ref,
    residual_hbm, w_out_hbm,
    stream, normed, routes, most,
    tail_out, tails, run_out, far, diff_out, parts, route_own, most_out, most_in,
    resid, mapped, w_out,
    load_sem, tail_send, tail_recv, far_send, far_recv, diff_send, diff_recv,
    most_send, most_recv, route_send, route_recv,
):
    groups, channels, length = pool_ref.shape
    rows = length // tp_count
    lines = groups * channels
    chunks, _, wide = normed.shape
    sp, tp = lax.axis_index("sp"), lax.axis_index("tp")
    plane_size = sp_count // PLANES
    peers = plane_size * tp_count
    plane = sp // plane_size
    spot = sp - plane * plane_size
    last = PLANES - 1

    loads = []
    for i, (source, target) in enumerate(((residual_hbm, resid), (w_out_hbm, w_out))):
        copy = pltpu.make_async_copy(source, target, load_sem.at[i])
        copy.start()
        loads.append(copy)

    barrier = pltpu.get_barrier_semaphore()
    for i in range(1, sp_count):
        pl.semaphore_signal(
            barrier, inc=1, device_id=(lax.rem(sp + i, sp_count), tp), device_id_type=MESH
        )
    for i in range(1, tp_count):
        pl.semaphore_signal(
            barrier, inc=1, device_id=(sp, lax.rem(tp + i, tp_count)), device_id_type=MESH
        )

    route = jnp.concatenate([ids_ref[...].astype(F32), logits_ref[...]], axis=0)
    route_own[...] = route
    routes[plane] = route
    count = jnp.zeros((1, 1), F32)
    for edge in (0, last):
        bound = jnp.where(plane == edge, 0.0, jnp.sum(needed(route, edge, peers), axis=1, keepdims=True))
        count = jnp.maximum(count, bound)
    values = pool_ref[...].reshape(lines, length)
    doc = doc_ref[...].astype(F32)
    last_id = doc[:, length - 1 :]
    tail_mask = jnp.broadcast_to((doc == last_id).astype(BF16), (8, length))
    tail_sum = contract(tail_mask, values, 1, 1)[:1]
    tail_count = jnp.sum((doc == last_id).astype(F32), axis=1, keepdims=True)
    tail_row = jnp.concatenate(
        [
            tail_sum,
            jnp.broadcast_to(last_id, (1, 128)),
            jnp.broadcast_to(tail_count, (1, 128)),
            jnp.broadcast_to(count, (1, 128)),
        ],
        axis=1,
    )
    tail_out[...] = tail_row
    tails[sp] = tail_row
    doc_col = jnp.broadcast_to(doc, (128, length)).T[:, :1]
    row_at = lax.broadcasted_iota(jnp.int32, (length, length), 0)
    col_at = lax.broadcasted_iota(jnp.int32, (length, length), 1)
    same = jnp.where((row_at <= col_at) & (doc_col == doc), 1.0, 0.0)
    local_count = jnp.sum(same, axis=0, keepdims=True)
    local_run = jnp.dot(values, same.astype(BF16), preferred_element_type=F32)
    run_out[...] = local_run.astype(BF16).reshape(groups, channels, length)
    pl.semaphore_wait(barrier, sp_count + tp_count - 2)
    early = [
        send(
            tail_out, tails.at[sp], tail_send.at[i], tail_recv.at[i],
            (lax.rem(sp + i, sp_count), tp),
        )
        for i in range(1, sp_count)
    ]
    early += [
        send(
            run_out.at[g], far.at[g], far_send.at[g], far_recv.at[g],
            (lax.rem(sp + 2**g, sp_count), tp),
        )
        for g in reversed(range(groups))
    ]
    route_copies = [
        send(
            route_own, routes.at[plane], route_send.at[i], route_recv.at[i],
            (lax.rem(plane + i, PLANES) * plane_size + spot, tp),
        )
        for i in range(1, PLANES)
    ]

    for copy in early:
        copy.wait()
    table = jnp.concatenate([tails[j] for j in range(sp_count)], axis=0)
    sources = lax.broadcasted_iota(jnp.int32, (sp_count, 1), 0)
    joined = jnp.where((sources < sp) & (table[:, lines : lines + 1] == doc), 1.0, 0.0)
    position = local_count + jnp.sum(
        joined * table[:, lines + 128 : lines + 129], axis=0, keepdims=True
    )
    for g in range(groups):
        span = float(length * 2**g)
        at = slice(g * channels, (g + 1) * channels)
        between = contract(
            table[:, at], jnp.where(sources >= sp - 2**g, joined, 0.0), 0, 0,
            precision=lax.Precision.HIGHEST,
        )
        window = local_run[at] + between - jnp.where(position > span, far[g].astype(F32), 0.0)
        diff = window / jnp.minimum(position, span) - values[at].astype(F32)
        diff = diff.astype(BF16)
        for q in range(tp_count):
            diff_out[q, g] = diff[:, q * rows : (q + 1) * rows]
    parts[tp] = diff_out[tp]
    most_out[...] = jnp.broadcast_to(
        jnp.max(table[:, lines + 256 : lines + 257], axis=0, keepdims=True), (1, 128)
    )
    most_in[tp] = most_out[...]
    diff_copies = []
    for i in range(1, tp_count):
        other = lax.rem(tp + i, tp_count)
        diff_copies.append(
            send(diff_out.at[other], parts.at[tp], diff_send.at[i], diff_recv.at[i], (sp, other))
        )
        diff_copies.append(
            send(most_out, most_in.at[tp], most_send.at[i], most_recv.at[i], (sp, other))
        )
    loads[0].wait()
    loads[1].wait()
    for copy in diff_copies:
        copy.wait()
    for g in range(groups):
        channel_rows = jnp.concatenate([parts[q, g] for q in range(tp_count)], axis=0)
        size = tp_count * channels
        at = slice(g * size, (g + 1) * size)
        mapped[:, at] = (contract(channel_rows, map_ref[g], 0, 0) * scale_ref[:, at]).astype(BF16)

    step = min(rows, 128)

    def norm_rows(i, carry):
        at = pl.ds(pl.multiple_of(i * step, step), step)
        projected = jnp.dot(mapped[at, :], w_out[...], preferred_element_type=F32)
        line = (
            resid[at, :].astype(F32) + mix_ref[...] * projected * rms_scale(projected)
        ).astype(BF16)
        stream[at, :] = line
        back = line.astype(F32)
        ready = (ffn_ref[...] * back * rms_scale(back)).astype(BF16)
        for c in range(chunks):
            normed[c, at, :] = ready[:, c * wide : (c + 1) * wide]
        return carry

    lax.fori_loop(0, rows // step, norm_rows, 0)

    top = most_in[0]
    for q in range(1, tp_count):
        top = jnp.maximum(top, most_in[q])
    most[...] = top.astype(jnp.int32)
    for copy in route_copies:
        copy.wait()


def needed(route, edge, peers):
    first, second = route[0:1], route[1:2]
    low, high = edge * peers, (edge + 1) * peers
    if not isinstance(edge, int):
        low, high = low.astype(F32), high.astype(F32)
    return jnp.where(
        ((first >= low) & (first < high)) | ((second >= low) & (second < high)), 1.0, 0.0
    )


def layer_kernel(
    sp_count, tp_count,
    normed_own, routes, gain_ref, stream_hbm, w_gate_hbm, w_up_hbm, w_down_hbm,
    out_ref,
    stream, w_gate, w_up, w_down,
    normed, picked, mix_high, mix_low, packs, forward,
    outgoing, arrived, hidden, results, total, partial_out, partial_in,
    load_sem, near_send, edge_send, line_recv,
    out_send, out_recv, back_send, back_recv, part_send, part_recv,
):
    chunks, rows, wide = normed_own.shape
    peers, capacity = outgoing.shape[2], outgoing.shape[3]
    slots = peers * capacity
    packed = packs.shape[1]
    depth, _, tile = hidden.shape
    sp, tp = lax.axis_index("sp"), lax.axis_index("tp")
    plane_size = sp_count // PLANES
    plane = sp // plane_size
    spot = sp - plane * plane_size
    me = spot * tp_count + tp
    last = PLANES - 1
    outer = (plane == 0) | (plane == last)
    edge = jnp.where(plane <= 1, 0, last)
    inner = jnp.where(plane <= 1, 1 + plane, plane - 1)
    visits = [
        sum((plane == q).astype(jnp.int32) * s for q, s in enumerate(column))
        for column in zip(*VISITS)
    ]

    def in_line(other):
        return (other * plane_size + spot, tp)

    loads = []
    for i, (source, target) in enumerate((
        (w_gate_hbm.at[0], w_gate), (w_up_hbm.at[0], w_up), (w_down_hbm.at[0], w_down),
        (stream_hbm, stream),
    )):
        copy = pltpu.make_async_copy(source, target, load_sem.at[i])
        copy.start()
        loads.append(copy)

    barrier = pltpu.get_barrier_semaphore()
    for i in range(1, PLANES):
        pl.semaphore_signal(
            barrier, inc=1, device_id=in_line(lax.rem(plane + i, PLANES)), device_id_type=MESH
        )
    for i in range(1, peers):
        peer = lax.rem(me + i, peers)
        pl.semaphore_signal(
            barrier, inc=1,
            device_id=(plane * plane_size + peer // tp_count, lax.rem(peer, tp_count)),
            device_id_type=MESH,
        )

    expand = (
        lax.broadcasted_iota(jnp.int32, (slots, peers), 0) // capacity
        == lax.broadcasted_iota(jnp.int32, (slots, peers), 1)
    ).astype(BF16)
    at_row = lax.broadcasted_iota(jnp.int32, (rows, rows), 0)
    at_col = lax.broadcasted_iota(jnp.int32, (rows, rows), 1)
    earlier = (at_row < at_col).astype(BF16)
    slot_down = lax.rem(lax.broadcasted_iota(jnp.int32, (slots, rows), 0), capacity).astype(F32)
    slot_across = lax.rem(lax.broadcasted_iota(jnp.int32, (rows, slots), 1), capacity).astype(F32)
    experts = (lax.broadcasted_iota(jnp.int32, (peers, rows), 0) + plane * peers).astype(F32)

    pack_down = lax.broadcasted_iota(jnp.int32, (packed, rows), 0).astype(F32)

    def place(block, compact, forwarded):
        route = routes[block]
        first, second = route[0:1] == experts, route[1:2] == experts
        named = jnp.where(first | second, 1.0, 0.0)
        rank = jnp.dot(named.astype(BF16), earlier, preferred_element_type=F32)
        code = jnp.where(named > 0.0, rank, -1.0).astype(BF16)
        chosen = jnp.where(
            jnp.dot(expand, code, preferred_element_type=F32) == slot_down, 1.0, 0.0
        ).astype(BF16)
        weight = jnp.where(first, jax.nn.sigmoid(route[2:3] - route[3:4]), 0.0) + jnp.where(
            second, jax.nn.sigmoid(route[3:4] - route[2:3]), 0.0
        )
        top = weight.astype(BF16)
        rest = (weight - top.astype(F32)).astype(BF16)
        here = contract(code, expand, 0, 1) == slot_across
        top = jnp.where(here, contract(top, expand, 0, 1), 0.0).astype(BF16)
        rest = jnp.where(here, contract(rest, expand, 0, 1), 0.0).astype(BF16)
        if compact or forwarded:
            need = jnp.broadcast_to(needed(route, edge, peers), (8, rows))
            turn = jnp.dot(need.astype(BF16), earlier, preferred_element_type=F32)
            turn = jnp.where(need > 0.0, turn, -1.0)[0:1]
            pack = jnp.where(turn == pack_down, 1.0, 0.0).astype(BF16)
            if forwarded:
                packs[block] = pack
        if compact:
            picked[block, :, 0:packed] = contract(chosen, pack, 1, 1).astype(BF16)
            mix_high[block, 0:packed] = jnp.dot(pack, top, preferred_element_type=F32).astype(BF16)
            mix_low[block, 0:packed] = jnp.dot(pack, rest, preferred_element_type=F32).astype(BF16)
        else:
            picked[block] = chosen
            mix_high[block] = top
            mix_low[block] = rest

    def to_inner(k, c):
        s = visits[k]
        source = normed_own.at[c] if k == 0 else normed.at[s, c]
        return remote(
            source, normed.at[s, c], near_send.at[k, c], line_recv.at[s, c], in_line(inner)
        )

    def to_edge(k, c):
        s = visits[k]
        return remote(
            forward.at[k, c], normed.at[s, c, pl.ds(0, packed)],
            edge_send.at[k, c], line_recv.at[s, c], in_line(edge),
        )

    def pack_edge(k, c):
        s = visits[k]
        source = normed_own[c] if k == 0 else normed[s, c]
        forward[k, c] = jnp.dot(packs[s], source, preferred_element_type=F32).astype(BF16)
        to_edge(k, c).start()

    def spread(source, target, send_sem, recv_sem, k, c):
        def body(i, carry):
            peer = lax.rem(me + i, peers)
            pltpu.make_async_remote_copy(
                src_ref=source.at[k, c, peer],
                dst_ref=target.at[k, c, me],
                send_sem=send_sem.at[k, c],
                recv_sem=recv_sem.at[k, c],
                device_id=(plane * plane_size + peer // tp_count, lax.rem(peer, tp_count)),
                device_id_type=MESH,
            ).start()
            return carry

        lax.fori_loop(1, peers, body, 0)
        target[k, c, me] = source[k, c, me]

    def settle(buffer, sem, k, c):
        whole = buffer.at[k, c, pl.ds(0, peers - 1)]
        pltpu.make_async_copy(whole, whole, sem.at[k, c]).wait()

    def every(body, first=0, end=4):
        def wrapped(c, carry):
            body(c)
            return carry

        lax.fori_loop(chunks * first // 4, chunks * end // 4, wrapped, 0)

    def fetch(k, c, height):
        ref = normed.at[visits[k], c, pl.ds(0, height)]
        pltpu.make_async_copy(ref, ref, line_recv.at[visits[k], c]).wait()

    def hand_out(k, c, height):
        s = visits[k]
        source = normed_own[c] if k == 0 else normed[s, c, 0:height]
        value = jnp.dot(picked[s, :, 0:height], source, preferred_element_type=F32)
        outgoing[k, c] = value.astype(BF16).reshape(peers, capacity, wide)
        spread(outgoing, arrived, out_send, out_recv, k, c)

    def give_out(k, c):
        spread(outgoing, results, back_send, back_recv, k, c)

    def run_expert(k, give):
        every(lambda c: settle(arrived, out_recv, k, c))

        def body(f, carry):
            at = pl.ds(pl.multiple_of(f * tile, tile), tile)
            gate = jnp.zeros((slots, tile), F32)
            up = jnp.zeros((slots, tile), F32)
            for c in range(chunks):
                line = arrived[k, c].reshape(slots, wide)
                inner = slice(c * wide, (c + 1) * wide)
                gate = gate + jnp.dot(line, w_gate[inner, at], preferred_element_type=F32)
                up = up + jnp.dot(line, w_up[inner, at], preferred_element_type=F32)
            hidden[f] = (jax.nn.silu(gate) * up).astype(BF16)
            return carry

        lax.fori_loop(0, depth, body, 0)

        def give_back(c):
            at = pl.ds(pl.multiple_of(c * wide, wide), wide)
            value = jnp.zeros((slots, wide), F32)
            for f in range(depth):
                inner = slice(f * tile, (f + 1) * tile)
                value = value + jnp.dot(hidden[f], w_down[inner, at], preferred_element_type=F32)
            settle(outgoing, out_send, k, c)
            outgoing[k, c] = value.astype(BF16).reshape(peers, capacity, wide)
            if give:
                give_out(k, c)

        every(give_back)

    def gathered(k, c, height):
        s = visits[k]
        settle(results, back_recv, k, c)
        line = results[k, c].reshape(slots, wide)
        return jnp.dot(mix_high[s, 0:height], line, preferred_element_type=F32) + jnp.dot(
            mix_low[s, 0:height], line, preferred_element_type=F32
        )

    def part_copy(k, c, height, target):
        s = visits[k]
        slot = jnp.where((s == target) & (target < plane), PLANES, s)
        at = pl.ds(0, height)
        return remote(
            partial_out.at[s, c, at], partial_in.at[slot, c, at],
            part_send.at[s, c], part_recv.at[slot, c], in_line(target),
        )

    def await_part(slot, c, height):
        ref = partial_in.at[slot, c, pl.ds(0, height)]
        pltpu.make_async_copy(ref, ref, part_recv.at[slot, c]).wait()

    def unpacked(s, slot, c):
        await_part(slot, c, packed)
        return contract(packs[s], partial_in[slot, c, 0:packed], 0, 0)

    def give_end(k, c):
        partial_out[visits[k], c, 0:packed] = gathered(k, c, packed).astype(BF16)
        part_copy(k, c, packed, inner).start()

    def give_far(k, c):
        s = visits[k]
        value = gathered(k, c, rows) + unpacked(s, s, c)
        partial_out[s, c] = value.astype(BF16)
        part_copy(k, c, rows, inner).start()

    def give_near(k, c):
        s = visits[k]
        value = gathered(k, c, rows)
        await_part(s, c, rows)
        partial_out[s, c] = (value + partial_in[s, c].astype(F32)).astype(BF16)
        part_copy(k, c, rows, edge).start()

    def own(c):
        total[c] = gathered(0, c, rows)

    def out_of(k, first=0, end=4):
        every(lambda c: give_out(k, c), first, end)

    def drain():
        for k in range(PLANES):
            every(lambda c: settle(outgoing, back_send, k, c))

    place(plane, False, True)
    pl.semaphore_wait(barrier, PLANES + peers - 2)

    @pl.when(outer)
    def _():
        def hand(k, first=0, end=4):
            def body(c):
                fetch(k, c, packed)
                hand_out(k, c, packed)

            every(body, first, end)

        def part(k, first=0, end=4):
            every(lambda c: give_end(k, c), first, end)

        every(lambda c: to_inner(0, c).start())
        every(lambda c: hand_out(0, c, rows))
        for k in range(1, PLANES):
            place(visits[k], True, False)
        for copy in loads[:3]:
            copy.wait()
        hand(1, 0, 1)
        run_expert(0, False)
        out_of(0, 0, 1)
        hand(1, 1, 2)
        out_of(0, 1, 2)
        hand(1, 2, 4)
        run_expert(1, True)
        hand(2, 0, 2)
        part(1, 0, 2)
        hand(2, 2, 3)
        part(1, 2, 4)
        hand(2, 3, 4)
        hand(3, 0, 2)
        run_expert(2, True)
        hand(3, 2, 4)
        part(2)
        run_expert(3, True)
        out_of(0, 2, 4)
        part(3)
        every(own)
        home = jnp.where(plane == 0, PLANES, plane)

        def finish(c):
            await_part(home, c, rows)
            total[c] = total[c] + partial_in[home, c].astype(F32)

        every(finish)
        every(lambda c: to_inner(0, c).wait_send())
        for k in range(1, PLANES):
            every(lambda c: part_copy(k, c, packed, inner).wait_send())

    @pl.when(jnp.logical_not(outer))
    def _():
        def hand_far(first, end):
            def body(c):
                fetch(3, c, rows)
                pack_edge(3, c)
                hand_out(3, c, rows)

            every(body, first, end)

        def both_in(c):
            fetch(2, c, rows)
            pack_edge(2, c)
            fetch(1, c, rows)
            to_inner(1, c).start()
            hand_out(2, c, rows)
            hand_out(1, c, rows)

        every(lambda c: to_inner(0, c).start())
        every(lambda c: pack_edge(0, c), 0, 2)
        every(lambda c: hand_out(0, c, rows), 0, 2)
        for k in range(1, PLANES):
            place(visits[k], False, k > 1)
        for copy in loads[:3]:
            copy.wait()
        every(both_in)
        hand_far(0, 1)
        run_expert(2, True)
        hand_far(1, 3)
        run_expert(1, False)
        hand_far(3, 4)
        every(lambda c: pack_edge(0, c), 2, 4)
        every(lambda c: hand_out(0, c, rows), 2, 4)
        out_of(1)
        every(lambda c: give_far(2, c))
        run_expert(3, True)
        run_expert(0, False)
        out_of(0)
        every(lambda c: give_far(3, c), 0, 2)
        every(lambda c: give_near(1, c), 0, 1)
        every(lambda c: give_far(3, c), 2, 3)
        every(lambda c: give_near(1, c), 1, 2)
        every(lambda c: give_far(3, c), 3, 4)
        every(lambda c: give_near(1, c), 2, 4)
        every(own)
        far_slot = jnp.where(edge == 0, plane, PLANES)
        near_slot = jnp.where(edge == 0, PLANES, plane)

        def finish(c):
            value = total[c] + unpacked(plane, far_slot, c)
            await_part(near_slot, c, rows)
            total[c] = value + partial_in[near_slot, c].astype(F32)

        every(finish)
        for k in (0, 1):
            every(lambda c: to_inner(k, c).wait_send())
        for k in (0, 2, 3):
            every(lambda c: to_edge(k, c).wait_send())
        for k in (2, 3):
            every(lambda c: part_copy(k, c, rows, inner).wait_send())
        every(lambda c: part_copy(1, c, rows, edge).wait_send())

    loads[3].wait()
    step = min(rows, 128)

    def finish(i, carry):
        at = pl.ds(pl.multiple_of(i * step, step), step)
        summed = jnp.concatenate([total[c, at, :] for c in range(chunks)], axis=1)
        out_ref[at, :] = (
            stream[at, :].astype(F32) + gain_ref[...] * summed * rms_scale(summed)
        ).astype(BF16)
        return carry

    lax.fori_loop(0, rows // step, finish, 0)
    drain()


def mixer(
    pool_input, doc_ids, pool_map, pool_scale, w_out, residual, mix_gain, ffn_gain,
    expert_ids, route_logits,
):
    groups, channels, length = pool_input.shape
    sp_count, tp_count = lax.axis_size("sp"), lax.axis_size("tp")
    rows, width = residual.shape
    top_count = expert_ids.shape[1]
    pool_width = w_out.shape[0]
    wide = width // CHUNKS
    tail_width = groups * channels + 384
    vmem = pl.BlockSpec(memory_space=pltpu.VMEM)
    hbm = pl.BlockSpec(memory_space=pl.ANY)
    dma = pltpu.SemaphoreType.DMA
    return pl.pallas_call(
        functools.partial(mixer_kernel, sp_count, tp_count),
        out_shape=(
            jax.ShapeDtypeStruct((rows, width), BF16),
            jax.ShapeDtypeStruct((CHUNKS, rows, wide), BF16),
            jax.ShapeDtypeStruct((PLANES, 2 * top_count, rows), F32),
            jax.ShapeDtypeStruct((1, 128), jnp.int32),
        ),
        in_specs=[vmem] * 8 + [hbm] * 2,
        out_specs=(vmem,) * 4,
        scratch_shapes=[
            pltpu.VMEM((1, tail_width), F32),
            pltpu.VMEM((sp_count, 1, tail_width), F32),
            pltpu.VMEM((groups, channels, length), BF16),
            pltpu.VMEM((groups, channels, length), BF16),
            pltpu.VMEM((tp_count, groups, channels, rows), BF16),
            pltpu.VMEM((tp_count, groups, channels, rows), BF16),
            pltpu.VMEM((2 * top_count, rows), F32),
            pltpu.VMEM((1, 128), F32),
            pltpu.VMEM((tp_count, 1, 128), F32),
            pltpu.VMEM((rows, width), BF16),
            pltpu.VMEM((rows, pool_width), BF16),
            pltpu.VMEM((pool_width, width), BF16),
            dma((2,)),
            dma((sp_count,)),
            dma((sp_count,)),
            dma((groups,)),
            dma((groups,)),
            dma((tp_count,)),
            dma((tp_count,)),
            dma((tp_count,)),
            dma((tp_count,)),
            dma((PLANES,)),
            dma((PLANES,)),
        ],
        compiler_params=pltpu.CompilerParams(
            collective_id=0, has_side_effects=True, vmem_limit_bytes=67043328
        ),
    )(
        pool_input,
        doc_ids.reshape(1, -1),
        pool_map,
        pool_scale.reshape(1, -1),
        mix_gain.reshape(1, -1),
        ffn_gain.reshape(1, -1),
        expert_ids.T,
        route_logits.T,
        residual,
        w_out,
    )


def expert_layer(packed, collective_id, normed, routes, out_gain, stream, w_gate, w_up, w_down):
    sp_count, tp_count = lax.axis_size("sp"), lax.axis_size("tp")
    _, rows, wide = normed.shape
    width, hidden_width = w_gate.shape[1], w_gate.shape[2]
    top_count = routes.shape[1] // 2
    experts = sp_count * tp_count
    peers = experts // PLANES
    capacity = max(16, 2 * rows * top_count // experts)
    slots = peers * capacity
    tile = 256
    vmem = pl.BlockSpec(memory_space=pltpu.VMEM)
    hbm = pl.BlockSpec(memory_space=pl.ANY)
    exchange = pltpu.VMEM((PLANES, CHUNKS, peers, capacity, wide), BF16)
    dma = pltpu.SemaphoreType.DMA
    each = dma((PLANES, CHUNKS))
    return pl.pallas_call(
        functools.partial(layer_kernel, sp_count, tp_count),
        out_shape=jax.ShapeDtypeStruct(stream.shape, BF16),
        in_specs=[vmem] * 3 + [hbm] * 4,
        out_specs=vmem,
        scratch_shapes=[
            pltpu.VMEM((rows, width), BF16),
            pltpu.VMEM((width, hidden_width), BF16),
            pltpu.VMEM((width, hidden_width), BF16),
            pltpu.VMEM((hidden_width, width), BF16),
            pltpu.VMEM((PLANES, CHUNKS, rows, wide), BF16),
            pltpu.VMEM((PLANES, slots, rows), BF16),
            pltpu.VMEM((PLANES, rows, slots), BF16),
            pltpu.VMEM((PLANES, rows, slots), BF16),
            pltpu.VMEM((PLANES, packed, rows), BF16),
            pltpu.VMEM((PLANES, CHUNKS, packed, wide), BF16),
            exchange,
            exchange,
            pltpu.VMEM((hidden_width // tile, slots, tile), BF16),
            exchange,
            pltpu.VMEM((CHUNKS, rows, wide), F32),
            pltpu.VMEM((PLANES, CHUNKS, rows, wide), BF16),
            pltpu.VMEM((PLANES + 1, CHUNKS, rows, wide), BF16),
            dma((4,)),
            each,
            each,
            each,
            each,
            each,
            each,
            each,
            each,
            dma((PLANES + 1, CHUNKS)),
        ],
        compiler_params=pltpu.CompilerParams(
            collective_id=collective_id, has_side_effects=True, vmem_limit_bytes=67043328
        ),
    )(normed, routes, out_gain.reshape(1, -1), stream, w_gate, w_up, w_down)


def local(
    pool_input, doc_ids, pool_map, pool_scale, w_out, residual, mix_gain, ffn_gain, out_gain,
    expert_ids, route_logits, w_gate, w_up, w_down,
):
    stream, normed, routes, most = mixer(
        pool_input, doc_ids, pool_map, pool_scale, w_out, residual, mix_gain, ffn_gain,
        expert_ids, route_logits,
    )
    rows = residual.shape[0]
    packed = 3 * rows // 4
    operands = (normed, routes, out_gain, stream, w_gate, w_up, w_down)
    return lax.cond(
        most[0, 0] <= packed,
        functools.partial(expert_layer, packed, 1),
        functools.partial(expert_layer, rows, 2),
        *operands,
    )


def solution(mesh):
    rows = P(("sp", "tp"), None)
    cubes = P(("sp", "tp"), None, None)
    in_specs = (
        P(None, "tp", "sp"), P("sp"), P(), P(), P(), rows, P(), P(), P(), rows, rows,
        cubes, cubes, cubes,
    )
    return jax.shard_map(local, mesh=mesh, in_specs=in_specs, out_specs=rows, check_vma=False)
```

```python
import functools
import jax
import jax.numpy as jnp
from jax import lax
from jax.sharding import PartitionSpec as P
from jax.experimental import pallas as pl
from jax.experimental.pallas import tpu as pltpu

MESH = pl.DeviceIdType.MESH
EPS = 1e-06
CHUNKS = 4
PLANES = 4
F32 = jnp.float32
BF16 = jnp.bfloat16


def rms_scale(vector):
    return lax.rsqrt(jnp.mean(vector * vector, axis=-1, keepdims=True) + EPS)


def contract(left, right, left_dim, right_dim, **options):
    return lax.dot_general(
        left, right, (((left_dim,), (right_dim,)), ((), ())), preferred_element_type=F32, **options
    )


VISITS = ((0, 2, 3, 1), (1, 0, 2, 3), (2, 3, 1, 0), (3, 1, 0, 2))


def remote(source, target, send_sem, recv_sem, device):
    return pltpu.make_async_remote_copy(
        src_ref=source,
        dst_ref=target,
        send_sem=send_sem,
        recv_sem=recv_sem,
        device_id=device,
        device_id_type=MESH,
    )


def send(*copy):
    made = remote(*copy)
    made.start()
    return made


def mixer_kernel(
    sp_count, tp_count,
    pool_ref, doc_ref, map_ref, scale_ref, mix_ref, ffn_ref, ids_ref, logits_ref,
    residual_hbm, w_out_hbm,
    stream, normed, routes, most,
    tail_out, tails, run_out, far, diff_out, parts, route_own, most_out, most_in,
    resid, mapped, w_out,
    load_sem, tail_send, tail_recv, far_send, far_recv, diff_send, diff_recv,
    most_send, most_recv, route_send, route_recv,
):
    groups, channels, length = pool_ref.shape
    rows = length // tp_count
    lines = groups * channels
    chunks, _, wide = normed.shape
    sp, tp = lax.axis_index("sp"), lax.axis_index("tp")
    plane_size = sp_count // PLANES
    peers = plane_size * tp_count
    plane = sp // plane_size
    spot = sp - plane * plane_size
    last = PLANES - 1

    loads = []
    for i, (source, target) in enumerate(((residual_hbm, resid), (w_out_hbm, w_out))):
        copy = pltpu.make_async_copy(source, target, load_sem.at[i])
        copy.start()
        loads.append(copy)

    barrier = pltpu.get_barrier_semaphore()
    for i in range(1, sp_count):
        pl.semaphore_signal(
            barrier, inc=1, device_id=(lax.rem(sp + i, sp_count), tp), device_id_type=MESH
        )
    for i in range(1, tp_count):
        pl.semaphore_signal(
            barrier, inc=1, device_id=(sp, lax.rem(tp + i, tp_count)), device_id_type=MESH
        )

    route = jnp.concatenate([ids_ref[...].astype(F32), logits_ref[...]], axis=0)
    route_own[...] = route
    routes[plane] = route
    count = jnp.zeros((1, 1), F32)
    for edge in (0, last):
        bound = jnp.where(plane == edge, 0.0, jnp.sum(needed(route, edge, peers), axis=1, keepdims=True))
        count = jnp.maximum(count, bound)
    values = pool_ref[...].reshape(lines, length)
    doc = doc_ref[...].astype(F32)
    last_id = doc[:, length - 1 :]
    tail_mask = jnp.broadcast_to((doc == last_id).astype(BF16), (8, length))
    tail_sum = contract(tail_mask, values, 1, 1)[:1]
    tail_count = jnp.sum((doc == last_id).astype(F32), axis=1, keepdims=True)
    tail_row = jnp.concatenate(
        [
            tail_sum,
            jnp.broadcast_to(last_id, (1, 128)),
            jnp.broadcast_to(tail_count, (1, 128)),
            jnp.broadcast_to(count, (1, 128)),
        ],
        axis=1,
    )
    tail_out[...] = tail_row
    tails[sp] = tail_row
    doc_col = jnp.broadcast_to(doc, (128, length)).T[:, :1]
    row_at = lax.broadcasted_iota(jnp.int32, (length, length), 0)
    col_at = lax.broadcasted_iota(jnp.int32, (length, length), 1)
    same = jnp.where((row_at <= col_at) & (doc_col == doc), 1.0, 0.0)
    local_count = jnp.sum(same, axis=0, keepdims=True)
    local_run = jnp.dot(values, same.astype(BF16), preferred_element_type=F32)
    run_out[...] = local_run.astype(BF16).reshape(groups, channels, length)
    pl.semaphore_wait(barrier, sp_count + tp_count - 2)
    early = [
        send(
            tail_out, tails.at[sp], tail_send.at[i], tail_recv.at[i],
            (lax.rem(sp + i, sp_count), tp),
        )
        for i in range(1, sp_count)
    ]
    early += [
        send(
            run_out.at[g], far.at[g], far_send.at[g], far_recv.at[g],
            (lax.rem(sp + 2**g, sp_count), tp),
        )
        for g in reversed(range(groups))
    ]
    route_copies = [
        send(
            route_own, routes.at[plane], route_send.at[i], route_recv.at[i],
            (lax.rem(plane + i, PLANES) * plane_size + spot, tp),
        )
        for i in range(1, PLANES)
    ]

    for copy in early:
        copy.wait()
    table = jnp.concatenate([tails[j] for j in range(sp_count)], axis=0)
    sources = lax.broadcasted_iota(jnp.int32, (sp_count, 1), 0)
    joined = jnp.where((sources < sp) & (table[:, lines : lines + 1] == doc), 1.0, 0.0)
    position = local_count + jnp.sum(
        joined * table[:, lines + 128 : lines + 129], axis=0, keepdims=True
    )
    for g in range(groups):
        span = float(length * 2**g)
        at = slice(g * channels, (g + 1) * channels)
        between = contract(
            table[:, at], jnp.where(sources >= sp - 2**g, joined, 0.0), 0, 0,
            precision=lax.Precision.HIGHEST,
        )
        window = local_run[at] + between - jnp.where(position > span, far[g].astype(F32), 0.0)
        diff = window / jnp.minimum(position, span) - values[at].astype(F32)
        diff = diff.astype(BF16)
        for q in range(tp_count):
            diff_out[q, g] = diff[:, q * rows : (q + 1) * rows]
    parts[tp] = diff_out[tp]
    most_out[...] = jnp.broadcast_to(
        jnp.max(table[:, lines + 256 : lines + 257], axis=0, keepdims=True), (1, 128)
    )
    most_in[tp] = most_out[...]
    diff_copies = []
    for i in range(1, tp_count):
        other = lax.rem(tp + i, tp_count)
        diff_copies.append(
            send(diff_out.at[other], parts.at[tp], diff_send.at[i], diff_recv.at[i], (sp, other))
        )
        diff_copies.append(
            send(most_out, most_in.at[tp], most_send.at[i], most_recv.at[i], (sp, other))
        )
    loads[0].wait()
    loads[1].wait()
    for copy in diff_copies:
        copy.wait()
    for g in range(groups):
        channel_rows = jnp.concatenate([parts[q, g] for q in range(tp_count)], axis=0)
        size = tp_count * channels
        at = slice(g * size, (g + 1) * size)
        mapped[:, at] = (contract(channel_rows, map_ref[g], 0, 0) * scale_ref[:, at]).astype(BF16)

    step = min(rows, 128)

    def norm_rows(i, carry):
        at = pl.ds(pl.multiple_of(i * step, step), step)
        projected = jnp.dot(mapped[at, :], w_out[...], preferred_element_type=F32)
        line = (
            resid[at, :].astype(F32) + mix_ref[...] * projected * rms_scale(projected)
        ).astype(BF16)
        stream[at, :] = line
        back = line.astype(F32)
        ready = (ffn_ref[...] * back * rms_scale(back)).astype(BF16)
        for c in range(chunks):
            normed[c, at, :] = ready[:, c * wide : (c + 1) * wide]
        return carry

    lax.fori_loop(0, rows // step, norm_rows, 0)

    top = most_in[0]
    for q in range(1, tp_count):
        top = jnp.maximum(top, most_in[q])
    most[...] = top.astype(jnp.int32)
    for copy in route_copies:
        copy.wait()


def needed(route, edge, peers):
    first, second = route[0:1], route[1:2]
    low, high = edge * peers, (edge + 1) * peers
    if not isinstance(edge, int):
        low, high = low.astype(F32), high.astype(F32)
    return jnp.where(
        ((first >= low) & (first < high)) | ((second >= low) & (second < high)), 1.0, 0.0
    )


def layer_kernel(
    sp_count, tp_count,
    normed_own, routes, gain_ref, stream_hbm, w_gate_hbm, w_up_hbm, w_down_hbm,
    out_ref,
    stream, w_gate, w_up, w_down,
    normed, picked, mix_high, mix_low, packs, forward,
    outgoing, arrived, gate_sum, up_sum, hidden, results, total, partial_out, partial_in,
    load_sem, near_send, edge_send, line_recv,
    out_send, out_recv, back_send, back_recv, part_send, part_recv,
):
    chunks, rows, wide = normed_own.shape
    peers, capacity = outgoing.shape[2], outgoing.shape[3]
    slots = peers * capacity
    packed = packs.shape[1]
    depth, _, tile = hidden.shape
    sp, tp = lax.axis_index("sp"), lax.axis_index("tp")
    plane_size = sp_count // PLANES
    plane = sp // plane_size
    spot = sp - plane * plane_size
    me = spot * tp_count + tp
    last = PLANES - 1
    outer = (plane == 0) | (plane == last)
    edge = jnp.where(plane <= 1, 0, last)
    inner = jnp.where(plane <= 1, 1 + plane, plane - 1)
    visits = [
        sum((plane == q).astype(jnp.int32) * s for q, s in enumerate(column))
        for column in zip(*VISITS)
    ]

    def in_line(other):
        return (other * plane_size + spot, tp)

    loads = []
    for i, (source, target) in enumerate((
        (w_gate_hbm.at[0], w_gate), (w_up_hbm.at[0], w_up), (w_down_hbm.at[0], w_down),
        (stream_hbm, stream),
    )):
        copy = pltpu.make_async_copy(source, target, load_sem.at[i])
        copy.start()
        loads.append(copy)

    barrier = pltpu.get_barrier_semaphore()
    for i in range(1, PLANES):
        pl.semaphore_signal(
            barrier, inc=1, device_id=in_line(lax.rem(plane + i, PLANES)), device_id_type=MESH
        )
    for i in range(1, peers):
        peer = lax.rem(me + i, peers)
        pl.semaphore_signal(
            barrier, inc=1,
            device_id=(plane * plane_size + peer // tp_count, lax.rem(peer, tp_count)),
            device_id_type=MESH,
        )

    expand = (
        lax.broadcasted_iota(jnp.int32, (slots, peers), 0) // capacity
        == lax.broadcasted_iota(jnp.int32, (slots, peers), 1)
    ).astype(BF16)
    at_row = lax.broadcasted_iota(jnp.int32, (rows, rows), 0)
    at_col = lax.broadcasted_iota(jnp.int32, (rows, rows), 1)
    earlier = (at_row < at_col).astype(BF16)
    slot_down = lax.rem(lax.broadcasted_iota(jnp.int32, (slots, rows), 0), capacity).astype(F32)
    slot_across = lax.rem(lax.broadcasted_iota(jnp.int32, (rows, slots), 1), capacity).astype(F32)
    experts = (lax.broadcasted_iota(jnp.int32, (peers, rows), 0) + plane * peers).astype(F32)

    pack_down = lax.broadcasted_iota(jnp.int32, (packed, rows), 0).astype(F32)

    def place(block, compact, forwarded):
        route = routes[block]
        first, second = route[0:1] == experts, route[1:2] == experts
        named = jnp.where(first | second, 1.0, 0.0)
        rank = jnp.dot(named.astype(BF16), earlier, preferred_element_type=F32)
        code = jnp.where(named > 0.0, rank, -1.0).astype(BF16)
        chosen = jnp.where(
            jnp.dot(expand, code, preferred_element_type=F32) == slot_down, 1.0, 0.0
        ).astype(BF16)
        weight = jnp.where(first, jax.nn.sigmoid(route[2:3] - route[3:4]), 0.0) + jnp.where(
            second, jax.nn.sigmoid(route[3:4] - route[2:3]), 0.0
        )
        top = weight.astype(BF16)
        rest = (weight - top.astype(F32)).astype(BF16)
        here = contract(code, expand, 0, 1) == slot_across
        top = jnp.where(here, contract(top, expand, 0, 1), 0.0).astype(BF16)
        rest = jnp.where(here, contract(rest, expand, 0, 1), 0.0).astype(BF16)
        if compact or forwarded:
            need = jnp.broadcast_to(needed(route, edge, peers), (8, rows))
            turn = jnp.dot(need.astype(BF16), earlier, preferred_element_type=F32)
            turn = jnp.where(need > 0.0, turn, -1.0)[0:1]
            pack = jnp.where(turn == pack_down, 1.0, 0.0).astype(BF16)
            if forwarded:
                packs[block] = pack
        if compact:
            picked[block, :, 0:packed] = contract(chosen, pack, 1, 1).astype(BF16)
            mix_high[block, 0:packed] = jnp.dot(pack, top, preferred_element_type=F32).astype(BF16)
            mix_low[block, 0:packed] = jnp.dot(pack, rest, preferred_element_type=F32).astype(BF16)
        else:
            picked[block] = chosen
            mix_high[block] = top
            mix_low[block] = rest

    def to_inner(k, c):
        s = visits[k]
        source = normed_own.at[c] if k == 0 else normed.at[s, c]
        return remote(
            source, normed.at[s, c], near_send.at[k, c], line_recv.at[s, c], in_line(inner)
        )

    def to_edge(k, c):
        s = visits[k]
        return remote(
            forward.at[k, c], normed.at[s, c, pl.ds(0, packed)],
            edge_send.at[k, c], line_recv.at[s, c], in_line(edge),
        )

    def pack_edge(k, c):
        s = visits[k]
        source = normed_own[c] if k == 0 else normed[s, c]
        forward[k, c] = jnp.dot(packs[s], source, preferred_element_type=F32).astype(BF16)
        to_edge(k, c).start()

    def spread(source, target, send_sem, recv_sem, k, c):
        def body(i, carry):
            peer = lax.rem(me + i, peers)
            pltpu.make_async_remote_copy(
                src_ref=source.at[k, c, peer],
                dst_ref=target.at[k, c, me],
                send_sem=send_sem.at[k, c],
                recv_sem=recv_sem.at[k, c],
                device_id=(plane * plane_size + peer // tp_count, lax.rem(peer, tp_count)),
                device_id_type=MESH,
            ).start()
            return carry

        lax.fori_loop(1, peers, body, 0)
        target[k, c, me] = source[k, c, me]

    def settle(buffer, sem, k, c):
        whole = buffer.at[k, c, pl.ds(0, peers - 1)]
        pltpu.make_async_copy(whole, whole, sem.at[k, c]).wait()

    def every(body, first=0, end=4):
        def wrapped(c, carry):
            body(c)
            return carry

        lax.fori_loop(chunks * first // 4, chunks * end // 4, wrapped, 0)

    def fetch(k, c, height):
        ref = normed.at[visits[k], c, pl.ds(0, height)]
        pltpu.make_async_copy(ref, ref, line_recv.at[visits[k], c]).wait()

    def hand_out(k, c, height):
        s = visits[k]
        source = normed_own[c] if k == 0 else normed[s, c, 0:height]
        value = jnp.dot(picked[s, :, 0:height], source, preferred_element_type=F32)
        outgoing[k, c] = value.astype(BF16).reshape(peers, capacity, wide)
        spread(outgoing, arrived, out_send, out_recv, k, c)

    def give_out(k, c):
        spread(outgoing, results, back_send, back_recv, k, c)

    def first_half(k):
        every(lambda c: settle(arrived, out_recv, k, c))

        def body(f, carry):
            at = pl.ds(pl.multiple_of(f * tile, tile), tile)
            gate = jnp.zeros((slots, tile), F32)
            up = jnp.zeros((slots, tile), F32)
            for c in range(chunks):
                line = arrived[k, c].reshape(slots, wide)
                inner = slice(c * wide, (c + 1) * wide)
                gate = gate + jnp.dot(line, w_gate[inner, at], preferred_element_type=F32)
                up = up + jnp.dot(line, w_up[inner, at], preferred_element_type=F32)
            hidden[f] = (jax.nn.silu(gate) * up).astype(BF16)
            return carry

        lax.fori_loop(0, depth, body, 0)

    def first_half_by_chunk(k):
        gate_sum[...] = jnp.zeros_like(gate_sum)
        up_sum[...] = jnp.zeros_like(up_sum)

        def take(c, finish):
            settle(arrived, out_recv, k, c)
            inner = pl.ds(pl.multiple_of(c * wide, wide), wide)

            def body(f, carry):
                at = pl.ds(pl.multiple_of(f * tile, tile), tile)
                line = arrived[k, c].reshape(slots, wide)
                gate = gate_sum[f] + jnp.dot(
                    line, w_gate[inner, at], preferred_element_type=F32
                )
                up = up_sum[f] + jnp.dot(line, w_up[inner, at], preferred_element_type=F32)
                if finish:
                    hidden[f] = (jax.nn.silu(gate) * up).astype(BF16)
                else:
                    gate_sum[f] = gate
                    up_sum[f] = up
                return carry

            lax.fori_loop(0, depth, body, 0)

        every(lambda c: take(c, False), 0, 3)
        take(chunks - 1, True)

    def run_expert(k, give, by_chunk=False):
        if by_chunk:
            first_half_by_chunk(k)
        else:
            first_half(k)

        def give_back(c):
            at = pl.ds(pl.multiple_of(c * wide, wide), wide)
            value = jnp.zeros((slots, wide), F32)
            for f in range(depth):
                inner = slice(f * tile, (f + 1) * tile)
                value = value + jnp.dot(hidden[f], w_down[inner, at], preferred_element_type=F32)
            settle(outgoing, out_send, k, c)
            outgoing[k, c] = value.astype(BF16).reshape(peers, capacity, wide)
            if give:
                give_out(k, c)

        every(give_back)

    def gathered(k, c, height):
        s = visits[k]
        settle(results, back_recv, k, c)
        line = results[k, c].reshape(slots, wide)
        return jnp.dot(mix_high[s, 0:height], line, preferred_element_type=F32) + jnp.dot(
            mix_low[s, 0:height], line, preferred_element_type=F32
        )

    def part_copy(k, c, height, target):
        s = visits[k]
        slot = jnp.where((s == target) & (target < plane), PLANES, s)
        at = pl.ds(0, height)
        return remote(
            partial_out.at[s, c, at], partial_in.at[slot, c, at],
            part_send.at[s, c], part_recv.at[slot, c], in_line(target),
        )

    def await_part(slot, c, height):
        ref = partial_in.at[slot, c, pl.ds(0, height)]
        pltpu.make_async_copy(ref, ref, part_recv.at[slot, c]).wait()

    def unpacked(s, slot, c):
        await_part(slot, c, packed)
        return contract(packs[s], partial_in[slot, c, 0:packed], 0, 0)

    def give_end(k, c):
        partial_out[visits[k], c, 0:packed] = gathered(k, c, packed).astype(BF16)
        part_copy(k, c, packed, inner).start()

    def give_far(k, c):
        s = visits[k]
        value = gathered(k, c, rows) + unpacked(s, s, c)
        partial_out[s, c] = value.astype(BF16)
        part_copy(k, c, rows, inner).start()

    def give_near(k, c):
        s = visits[k]
        value = gathered(k, c, rows)
        await_part(s, c, rows)
        partial_out[s, c] = (value + partial_in[s, c].astype(F32)).astype(BF16)
        part_copy(k, c, rows, edge).start()

    def own(c):
        total[c] = gathered(0, c, rows)

    def out_of(k, first=0, end=4):
        every(lambda c: give_out(k, c), first, end)

    def drain():
        for k in range(PLANES):
            every(lambda c: settle(outgoing, back_send, k, c))

    place(plane, False, True)
    pl.semaphore_wait(barrier, PLANES + peers - 2)

    @pl.when(outer)
    def _():
        def hand(k, first=0, end=4):
            def body(c):
                fetch(k, c, packed)
                hand_out(k, c, packed)

            every(body, first, end)

        def part(k, first=0, end=4):
            every(lambda c: give_end(k, c), first, end)

        every(lambda c: to_inner(0, c).start())
        every(lambda c: hand_out(0, c, rows))
        for k in range(1, PLANES):
            place(visits[k], True, False)
        for copy in loads[:3]:
            copy.wait()
        hand(1, 0, 1)
        run_expert(0, False)
        out_of(0, 0, 1)
        hand(1, 1, 2)
        out_of(0, 1, 2)
        hand(1, 2, 4)
        run_expert(1, True, True)
        hand(2, 0, 2)
        part(1, 0, 2)
        hand(2, 2, 3)
        part(1, 2, 4)
        hand(2, 3, 4)
        hand(3, 0, 2)
        run_expert(2, True, True)
        hand(3, 2, 4)
        part(2)
        run_expert(3, True, True)
        out_of(0, 2, 4)
        part(3)
        every(own)
        home = jnp.where(plane == 0, PLANES, plane)

        def finish(c):
            await_part(home, c, rows)
            total[c] = total[c] + partial_in[home, c].astype(F32)

        every(finish)
        every(lambda c: to_inner(0, c).wait_send())
        for k in range(1, PLANES):
            every(lambda c: part_copy(k, c, packed, inner).wait_send())

    @pl.when(jnp.logical_not(outer))
    def _():
        def hand_far(first, end):
            def body(c):
                fetch(3, c, rows)
                pack_edge(3, c)
                hand_out(3, c, rows)

            every(body, first, end)

        def both_in(c):
            fetch(2, c, rows)
            pack_edge(2, c)
            fetch(1, c, rows)
            to_inner(1, c).start()
            hand_out(2, c, rows)
            hand_out(1, c, rows)

        every(lambda c: to_inner(0, c).start())
        every(lambda c: pack_edge(0, c), 0, 2)
        every(lambda c: hand_out(0, c, rows), 0, 2)
        for k in range(1, PLANES):
            place(visits[k], False, k > 1)
        for copy in loads[:3]:
            copy.wait()
        every(both_in)
        hand_far(0, 1)
        run_expert(2, True)
        hand_far(1, 3)
        run_expert(1, False)
        hand_far(3, 4)
        every(lambda c: pack_edge(0, c), 2, 4)
        every(lambda c: hand_out(0, c, rows), 2, 4)
        out_of(1)
        every(lambda c: give_far(2, c))
        run_expert(3, True)
        run_expert(0, False)
        out_of(0)
        every(lambda c: give_far(3, c), 0, 2)
        every(lambda c: give_near(1, c), 0, 1)
        every(lambda c: give_far(3, c), 2, 3)
        every(lambda c: give_near(1, c), 1, 2)
        every(lambda c: give_far(3, c), 3, 4)
        every(lambda c: give_near(1, c), 2, 4)
        every(own)
        far_slot = jnp.where(edge == 0, plane, PLANES)
        near_slot = jnp.where(edge == 0, PLANES, plane)

        def finish(c):
            value = total[c] + unpacked(plane, far_slot, c)
            await_part(near_slot, c, rows)
            total[c] = value + partial_in[near_slot, c].astype(F32)

        every(finish)
        for k in (0, 1):
            every(lambda c: to_inner(k, c).wait_send())
        for k in (0, 2, 3):
            every(lambda c: to_edge(k, c).wait_send())
        for k in (2, 3):
            every(lambda c: part_copy(k, c, rows, inner).wait_send())
        every(lambda c: part_copy(1, c, rows, edge).wait_send())

    loads[3].wait()
    step = min(rows, 128)

    def finish(i, carry):
        at = pl.ds(pl.multiple_of(i * step, step), step)
        summed = jnp.concatenate([total[c, at, :] for c in range(chunks)], axis=1)
        out_ref[at, :] = (
            stream[at, :].astype(F32) + gain_ref[...] * summed * rms_scale(summed)
        ).astype(BF16)
        return carry

    lax.fori_loop(0, rows // step, finish, 0)
    drain()


def mixer(
    pool_input, doc_ids, pool_map, pool_scale, w_out, residual, mix_gain, ffn_gain,
    expert_ids, route_logits,
):
    groups, channels, length = pool_input.shape
    sp_count, tp_count = lax.axis_size("sp"), lax.axis_size("tp")
    rows, width = residual.shape
    top_count = expert_ids.shape[1]
    pool_width = w_out.shape[0]
    wide = width // CHUNKS
    tail_width = groups * channels + 384
    vmem = pl.BlockSpec(memory_space=pltpu.VMEM)
    hbm = pl.BlockSpec(memory_space=pl.ANY)
    dma = pltpu.SemaphoreType.DMA
    return pl.pallas_call(
        functools.partial(mixer_kernel, sp_count, tp_count),
        out_shape=(
            jax.ShapeDtypeStruct((rows, width), BF16),
            jax.ShapeDtypeStruct((CHUNKS, rows, wide), BF16),
            jax.ShapeDtypeStruct((PLANES, 2 * top_count, rows), F32),
            jax.ShapeDtypeStruct((1, 128), jnp.int32),
        ),
        in_specs=[vmem] * 8 + [hbm] * 2,
        out_specs=(vmem,) * 4,
        scratch_shapes=[
            pltpu.VMEM((1, tail_width), F32),
            pltpu.VMEM((sp_count, 1, tail_width), F32),
            pltpu.VMEM((groups, channels, length), BF16),
            pltpu.VMEM((groups, channels, length), BF16),
            pltpu.VMEM((tp_count, groups, channels, rows), BF16),
            pltpu.VMEM((tp_count, groups, channels, rows), BF16),
            pltpu.VMEM((2 * top_count, rows), F32),
            pltpu.VMEM((1, 128), F32),
            pltpu.VMEM((tp_count, 1, 128), F32),
            pltpu.VMEM((rows, width), BF16),
            pltpu.VMEM((rows, pool_width), BF16),
            pltpu.VMEM((pool_width, width), BF16),
            dma((2,)),
            dma((sp_count,)),
            dma((sp_count,)),
            dma((groups,)),
            dma((groups,)),
            dma((tp_count,)),
            dma((tp_count,)),
            dma((tp_count,)),
            dma((tp_count,)),
            dma((PLANES,)),
            dma((PLANES,)),
        ],
        compiler_params=pltpu.CompilerParams(
            collective_id=0, has_side_effects=True, vmem_limit_bytes=67043328
        ),
    )(
        pool_input,
        doc_ids.reshape(1, -1),
        pool_map,
        pool_scale.reshape(1, -1),
        mix_gain.reshape(1, -1),
        ffn_gain.reshape(1, -1),
        expert_ids.T,
        route_logits.T,
        residual,
        w_out,
    )


def expert_layer(packed, collective_id, normed, routes, out_gain, stream, w_gate, w_up, w_down):
    sp_count, tp_count = lax.axis_size("sp"), lax.axis_size("tp")
    _, rows, wide = normed.shape
    width, hidden_width = w_gate.shape[1], w_gate.shape[2]
    top_count = routes.shape[1] // 2
    experts = sp_count * tp_count
    peers = experts // PLANES
    capacity = max(16, 2 * rows * top_count // experts)
    slots = peers * capacity
    tile = 256
    vmem = pl.BlockSpec(memory_space=pltpu.VMEM)
    hbm = pl.BlockSpec(memory_space=pl.ANY)
    exchange = pltpu.VMEM((PLANES, CHUNKS, peers, capacity, wide), BF16)
    dma = pltpu.SemaphoreType.DMA
    each = dma((PLANES, CHUNKS))
    return pl.pallas_call(
        functools.partial(layer_kernel, sp_count, tp_count),
        out_shape=jax.ShapeDtypeStruct(stream.shape, BF16),
        in_specs=[vmem] * 3 + [hbm] * 4,
        out_specs=vmem,
        scratch_shapes=[
            pltpu.VMEM((rows, width), BF16),
            pltpu.VMEM((width, hidden_width), BF16),
            pltpu.VMEM((width, hidden_width), BF16),
            pltpu.VMEM((hidden_width, width), BF16),
            pltpu.VMEM((PLANES, CHUNKS, rows, wide), BF16),
            pltpu.VMEM((PLANES, slots, rows), BF16),
            pltpu.VMEM((PLANES, rows, slots), BF16),
            pltpu.VMEM((PLANES, rows, slots), BF16),
            pltpu.VMEM((PLANES, packed, rows), BF16),
            pltpu.VMEM((PLANES, CHUNKS, packed, wide), BF16),
            exchange,
            exchange,
            pltpu.VMEM((hidden_width // tile, slots, tile), F32),
            pltpu.VMEM((hidden_width // tile, slots, tile), F32),
            pltpu.VMEM((hidden_width // tile, slots, tile), BF16),
            exchange,
            pltpu.VMEM((CHUNKS, rows, wide), F32),
            pltpu.VMEM((PLANES, CHUNKS, rows, wide), BF16),
            pltpu.VMEM((PLANES + 1, CHUNKS, rows, wide), BF16),
            dma((4,)),
            each,
            each,
            each,
            each,
            each,
            each,
            each,
            each,
            dma((PLANES + 1, CHUNKS)),
        ],
        compiler_params=pltpu.CompilerParams(
            collective_id=collective_id, has_side_effects=True, vmem_limit_bytes=67043328
        ),
    )(normed, routes, out_gain.reshape(1, -1), stream, w_gate, w_up, w_down)


def local(
    pool_input, doc_ids, pool_map, pool_scale, w_out, residual, mix_gain, ffn_gain, out_gain,
    expert_ids, route_logits, w_gate, w_up, w_down,
):
    stream, normed, routes, most = mixer(
        pool_input, doc_ids, pool_map, pool_scale, w_out, residual, mix_gain, ffn_gain,
        expert_ids, route_logits,
    )
    rows = residual.shape[0]
    packed = 3 * rows // 4
    operands = (normed, routes, out_gain, stream, w_gate, w_up, w_down)
    return lax.cond(
        most[0, 0] <= packed,
        functools.partial(expert_layer, packed, 1),
        functools.partial(expert_layer, rows, 2),
        *operands,
    )


def solution(mesh):
    rows = P(("sp", "tp"), None)
    cubes = P(("sp", "tp"), None, None)
    in_specs = (
        P(None, "tp", "sp"), P("sp"), P(), P(), P(), rows, P(), P(), P(), rows, rows,
        cubes, cubes, cubes,
    )
    return jax.shard_map(local, mesh=mesh, in_specs=in_specs, out_specs=rows, check_vma=False)
```
